32 devices in a mesh: sp: 8 (over z, x), tp: 4 (over y, core).
Axes of the slice: x: 2, y: 2, z: 4, core: 2. Of those that a mesh axis runs over, the one named last changes fastest.
Arguments:
- result_cotangent_values: bfloat16 [1024, 2048], P('sp'), may hold values from -6 to 6
- specialist_entry_vectors: bfloat16 [1024, 2048], P('sp'), may hold values from -6 to 6
- chosen_specialists: int32 [1024, 2], P('sp'), may hold values from 0 to 3, all different within a row; in each aligned block of 128 rows (0 to 127, 128 to 255, ...) at most 128 rows name the same one
- specialist_mixing_shares: float32 [1024, 2], P('sp'), may hold values from 0.1 to 0.9
- specialist_switch_maps: bfloat16 [8, 2048, 1792], P('sp', None, 'tp'), may hold values from -0.125 to 0.125
- specialist_widen_maps: bfloat16 [8, 2048, 1792], P('sp', None, 'tp'), may hold values from -0.125 to 0.125
- specialist_shrink_maps: bfloat16 [8, 1792, 2048], P('sp', 'tp'), may hold values from -0.09375 to 0.09375
- memory_readout_map: bfloat16 [2048, 2048], P('sp', 'tp'), may hold values from -0.125 to 0.125
- memory_source_vectors: bfloat16 [1024, 2048], P('sp', 'tp'), may hold values from -6 to 6
- memory_hidden_values: bfloat16 [1024, 2048], P('sp', 'tp'), may hold values from -6 to 6
- feature_fading_speed: float32 [2048], P('tp'), may hold values from 1.6276042e-05 to 0.009
- extra_log_fading: float32 [1024], P('sp'), may hold values from -2.8 to 0
- memory_switch_tiles: bfloat16 [8, 256, 256], P('tp'), may hold values from -0.375 to 0.375
- entry_switch_tiles: bfloat16 [8, 256, 256], P('tp'), may hold values from -0.375 to 0.375
Outputs:
- gate_proj_grad: bfloat16 [8, 2048, 1792], P('sp', None, 'tp')
- up_proj_grad: bfloat16 [8, 2048, 1792], P('sp', None, 'tp')
- down_proj_grad: bfloat16 [8, 1792, 2048], P('sp', 'tp')
- out_proj_grad: float32 [2048, 2048], P('sp', 'tp')
- lru_input_grad: float32 [1024, 2048], P('sp', 'tp')
The draws below stay inside these ranges and needn't reach their ends.
Inputs may be any that keep to these rules, and one draw needn't show every extreme that they name: `chosen_specialists`: each token names two different experts; among the 128 tokens of one device no expert is named more than 128 times, a bound that some block reaches on some device.
All inputs are finite; a program needn't handle non-finite values.
Results may differ from the reference program's by a relative error of at most 0.009.
Values may be sent and summed in bfloat16 or wider, within the bound.
A program may use at most 128 MiB of HBM per device.

```python
import math
import jax
import jax.numpy as jnp
import numpy as np
from jax import lax

D = 2048
FE = 3584
BLOCKS = 8
SLICES = 2
TOPK = 2
TOK_DEV = 128
SEQ = 1024
BW = 256
EXPERTS = 4
CAPACITY = 128
FE_PART = 1792
PARTS_SIZE = 8
FE_DEV = 448
N_SP = 8
N_TP = 4


def draw_feature_fading_speed(key, part):
    pick_key, slow_key, fast_key = jax.random.split(key, 3)
    share = 0.5
    slow_mask = jax.random.uniform(pick_key, (D,), jnp.float32) < share
    slow_rate = jnp.exp(jax.random.uniform(slow_key, (D,), jnp.float32, jnp.log(0.02), jnp.log(0.25))) / SEQ
    fast_rate = jnp.exp(jax.random.uniform(fast_key, (D,), jnp.float32, jnp.log(0.005), jnp.log(0.0085)))
    return jnp.where(slow_mask, slow_rate, fast_rate)


def draw_extra_log_fading(key, part):
    where_key, size_key = jax.random.split(key)
    spots = jax.random.randint(where_key, (4,), 0, SEQ)
    keeping = jax.random.uniform(size_key, (4,), jnp.float32, 0.5, 0.8)
    hits = (jnp.arange(SEQ, dtype=jnp.int32)[:, None] == spots[None, :]).astype(jnp.float32)
    return jnp.sum(hits * jnp.log(keeping)[None, :], axis=1)


def spiked(values, key, source, target, shards_of, factor):
    def block_of(dim):
        return (jnp.arange(values.shape[dim]) // (values.shape[dim] // shards_of)).reshape((-1,) + (1,) * (values.ndim - 1 - dim))

    one_side = jax.random.permutation(key, shards_of)[block_of(target)]
    second = (block_of(target) + shards_of // 2) % shards_of
    return jnp.where((block_of(source) == one_side) | (block_of(source) == second), factor * values, values)


def level_of(stream_key, shape, cuts, low, top_value):
    def one(position, shards_of):
        heights = jax.random.uniform(jax.random.fold_in(jax.random.fold_in(stream_key, 6), position), (shards_of,), jnp.float32, low / len(cuts), top_value / len(cuts))
        return jnp.repeat(jnp.exp(heights), shape[position] // shards_of).reshape((-1,) + (1,) * (len(shape) - position - 1))

    factor_of = one(*cuts[0])
    for cut in cuts[1:]:
        factor_of = factor_of * one(*cut)
    return factor_of


def shared_out(rng, own, number, rows, count, top, reach, lean):
    order = jax.random.permutation(rng, count)
    heavy_load, ordinary = portions_of(count, rows * top, reach, lean, True), portions_of(count, rows * top, reach, lean, False)
    places = jnp.arange(count)

    def named(tallies, offset_by):
        used = int((tallies > 0).sum())
        fixed = max(1, used // 4)
        passed = fixed + (places - fixed + offset_by * (used - fixed)) % max(1, count - fixed)
        return jnp.zeros((count,), jnp.int32).at[order[jnp.where(places < fixed, places, passed)]].set(jnp.asarray(tallies, jnp.int32))

    tallies = jnp.where(number % 4 == 0, named(heavy_load, number // 4), named(ordinary, number - number // 4 - 1))
    mixed = jax.random.permutation(jax.random.fold_in(own, 3), count)
    donor, receiver = mixed[0:count // 2 * 2:2], mixed[1:count // 2 * 2:2]
    room = jnp.minimum(tallies[donor] - 1, reach - tallies[receiver]) // 2
    room = jnp.where((donor == order[0]) | (receiver == order[0]) | (tallies[receiver] == 0), 0, jnp.maximum(room, 0))
    passed = jax.random.randint(jax.random.fold_in(own, 4), (count // 2,), 0, 1 << 20) % (room + 1)
    tallies = tallies.at[donor].add(-passed).at[receiver].add(passed)
    items = jnp.searchsorted(jnp.cumsum(tallies), jnp.arange(rows * top), side="right").astype(jnp.int32)
    listing = items.reshape(top, rows).T
    listing = listing[jax.random.permutation(jax.random.fold_in(own, 1), rows)]
    offset_by = jax.random.randint(jax.random.fold_in(own, 2), (rows, 1), 0, top)
    return jnp.take_along_axis(listing, (jnp.arange(top)[None, :] + offset_by) % top, axis=1)


def portions_of(count, total, most, slope, full):
    weights = [(1 << 20) // math.isqrt(rank ** slope) + 1 for rank in range(1, count + 1)]
    largest = most if full else min(most, max(-(-total // count), total * weights[0] // sum(weights)))
    least = 1 if total - largest >= count - 1 else 0
    given, spare = [largest] + [least] * (count - 1), total - largest - least * (count - 1)
    while spare > 0:
        free = [i for i in range(1, count) if given[i] < largest] or [i for i in range(1, count) if given[i] < most]
        pool, remaining = sum([weights[i] for i in free]), spare
        for i in free:
            more = min(most - given[i], max(1, remaining * weights[i] // pool), spare)
            given[i] = given[i] + more
            spare = spare - more
    return np.array(given)


def scatter_about(key, dims, width, limit, pieces=(), held_as=jnp.bfloat16):
    result = jax.random.normal(key, dims, jnp.float32) * width
    if len(pieces) > 0:
        result = level_of(key, dims, pieces, -0.22, 0.18) * result
    return jnp.clip(result, min=-limit, max=limit).astype(held_as)


def bell_draw_with(key, extent, deviation, bound, shards, heavy, held_as=jnp.bfloat16):
    entries = deviation * jax.random.normal(key, extent, jnp.float32)
    if shards:
        entries = entries * level_of(key, extent, shards, -0.22, 0.18)
    return jnp.clip(spiked(entries, jax.random.fold_in(key, 3), *heavy), -bound, bound).astype(held_as)


def setup_inputs(seed: int = 0) -> dict:
    keys = jax.random.split(jax.random.key(seed), 15)
    result_cotangent_values = bell_draw_with(keys[0], (SEQ, D), 1.0, 6.0, ((0, 8),), (0, 1, 8, 2.0))
    specialist_entry_vectors = scatter_about(keys[1], (SEQ, D), 1.0, 6.0, ((0, 8),))
    chosen_specialists_keys = jax.random.split(jax.random.fold_in(keys[2], 1), SEQ // TOK_DEV)
    chosen_specialists_turns = jax.random.permutation(jax.random.fold_in(keys[2], 3), SEQ // TOK_DEV)
    chosen_specialists = jax.vmap(lambda own, number: shared_out(jax.random.fold_in(keys[2], 2), own, number, TOK_DEV, EXPERTS, TOPK, CAPACITY, 1))(chosen_specialists_keys, chosen_specialists_turns).reshape((SEQ, TOPK))
    specialist_mixing_shares = jnp.clip(0.1 + 0.79999997 * jax.random.uniform(keys[3], (SEQ, TOPK), jnp.float32) ** level_of(keys[3], (SEQ, TOPK), ((0, 8),), -0.2, 0.2), 0.1, 0.9)
    specialist_switch_maps = scatter_about(keys[4], (EXPERTS * SLICES, D, FE_PART), D ** -0.5, 0.125, ((0, 8), (2, 4)))
    specialist_widen_maps = scatter_about(keys[5], (EXPERTS * SLICES, D, FE_PART), D ** -0.5, 0.125, ((0, 8), (2, 4)))
    specialist_shrink_maps = scatter_about(keys[6], (EXPERTS * SLICES, FE_PART, D), FE ** -0.5, 0.09375, ((0, 8), (1, 4)))
    memory_readout_map = scatter_about(keys[7], (D, D), D ** -0.5, 0.125, ((0, 8), (1, 4)))
    memory_source_vectors = scatter_about(keys[8], (SEQ, D), 1.0, 6.0, ((0, 8), (1, 4)))
    memory_hidden_values = scatter_about(keys[9], (SEQ, D), 1.0, 6.0, ((0, 8), (1, 4)))
    feature_fading_speed = draw_feature_fading_speed(jax.random.fold_in(keys[14], 71), 0)
    extra_log_fading = draw_extra_log_fading(jax.random.fold_in(keys[14], 71), 0)
    memory_switch_tiles = scatter_about(keys[12], (BLOCKS, BW, BW), BW ** -0.5, 0.375, ((0, 4),))
    entry_switch_tiles = scatter_about(keys[13], (BLOCKS, BW, BW), BW ** -0.5, 0.375, ((0, 4),))
    return dict(result_cotangent_values=result_cotangent_values, specialist_entry_vectors=specialist_entry_vectors, chosen_specialists=chosen_specialists, specialist_mixing_shares=specialist_mixing_shares, specialist_switch_maps=specialist_switch_maps, specialist_widen_maps=specialist_widen_maps, specialist_shrink_maps=specialist_shrink_maps, memory_readout_map=memory_readout_map, memory_source_vectors=memory_source_vectors, memory_hidden_values=memory_hidden_values, feature_fading_speed=feature_fading_speed, extra_log_fading=extra_log_fading, memory_switch_tiles=memory_switch_tiles, entry_switch_tiles=entry_switch_tiles)


def silu_slope(value):
    sig_value = jax.nn.sigmoid(value)
    return sig_value * (1.0 + value * (1.0 - sig_value))

def compose(upper_map, lower_map):
    return (lower_map[0] * upper_map[0], lower_map[1] + lower_map[0] * upper_map[1])

def slot_index(chosen_specialists):
    flat_expert = chosen_specialists.reshape(N_SP, TOPK * TOK_DEV)
    onehot = (flat_expert[:, :, None] == jnp.arange(EXPERTS, dtype=jnp.int32)[None, None, :]).astype(jnp.int32)
    slot_rank = lax.optimization_barrier(jnp.sum((jnp.cumsum(onehot, axis=1) - 1) * onehot, axis=2))
    source = jnp.arange(N_SP, dtype=jnp.int32)[:, None]
    index = (flat_expert * N_SP + source) * CAPACITY + slot_rank
    return index.reshape(-1).astype(jnp.int32)

def expert_pass(args):
    inputs, grads_in, gate_weight, up_weight, down_weight = args
    x_val = inputs.astype(jnp.float32)
    y_val = grads_in.astype(jnp.float32)
    gate_full = gate_weight.astype(jnp.float32)
    up_full = up_weight.astype(jnp.float32)
    down_full = down_weight.astype(jnp.float32)
    gate_value = jnp.einsum('rd,pdf->prf', x_val, gate_full)
    up_value = jnp.einsum('rd,pdf->prf', x_val, up_full)
    active = jax.nn.silu(gate_value)
    hidden = lax.optimization_barrier((active * up_value).astype(jnp.bfloat16)).astype(jnp.float32)
    down_grad = jnp.einsum('prf,rd->pfd', hidden, y_val).astype(jnp.bfloat16)
    hidden_grad = jnp.einsum('rd,pfd->prf', y_val, down_full)
    gate_grad = lax.optimization_barrier((hidden_grad * up_value * silu_slope(gate_value)).astype(jnp.bfloat16)).astype(jnp.float32)
    up_grad = lax.optimization_barrier((hidden_grad * active).astype(jnp.bfloat16)).astype(jnp.float32)
    gate_weight_grad = jnp.einsum('rd,prf->pdf', x_val, gate_grad).astype(jnp.bfloat16)
    up_weight_grad = jnp.einsum('rd,prf->pdf', x_val, up_grad).astype(jnp.bfloat16)
    token_part = jnp.einsum('prf,pdf->prd', gate_grad, gate_full) + jnp.einsum('prf,pdf->prd', up_grad, up_full)
    rounded = lax.optimization_barrier(token_part.astype(jnp.bfloat16)).astype(jnp.float32)
    return (gate_weight_grad, up_weight_grad, down_grad, lax.optimization_barrier(jnp.sum(rounded, axis=0)))

def reference(result_cotangent_values, specialist_entry_vectors, chosen_specialists, specialist_mixing_shares, specialist_switch_maps, specialist_widen_maps, specialist_shrink_maps, memory_readout_map, memory_source_vectors, memory_hidden_values, feature_fading_speed, extra_log_fading, memory_switch_tiles, entry_switch_tiles):
    index = slot_index(chosen_specialists)
    sent = (specialist_mixing_shares[:, :, None] * result_cotangent_values[:, None, :].astype(jnp.float32)).astype(jnp.bfloat16).reshape(SEQ * TOPK, D)
    copies = jnp.broadcast_to(specialist_entry_vectors[:, None, :], (SEQ, TOPK, D)).reshape(SEQ * TOPK, D)
    total_rows = EXPERTS * N_SP * CAPACITY
    grads_in = jnp.zeros((total_rows, D), jnp.bfloat16).at[index].set(sent).reshape(EXPERTS, N_SP * CAPACITY, D)
    inputs = jnp.zeros((total_rows, D), jnp.bfloat16).at[index].set(copies).reshape(EXPERTS, N_SP * CAPACITY, D)
    gate_parts = specialist_switch_maps.reshape(EXPERTS, SLICES, D, N_TP, FE_DEV).transpose(0, 1, 3, 2, 4).reshape(EXPERTS, PARTS_SIZE, D, FE_DEV)
    up_parts = specialist_widen_maps.reshape(EXPERTS, SLICES, D, N_TP, FE_DEV).transpose(0, 1, 3, 2, 4).reshape(EXPERTS, PARTS_SIZE, D, FE_DEV)
    down_parts = specialist_shrink_maps.reshape(EXPERTS, PARTS_SIZE, FE_DEV, D)
    gate_grads, up_grads, down_grads, partials = lax.map(expert_pass, (inputs, grads_in, gate_parts, up_parts, down_parts))
    moe_grad = jnp.take(partials.reshape(total_rows, D), index, axis=0).reshape(SEQ, TOPK, D).sum(axis=1)
    mixed_grad = (result_cotangent_values.astype(jnp.float32) + moe_grad).astype(jnp.bfloat16)
    upstream = jnp.dot(mixed_grad, memory_readout_map, preferred_element_type=jnp.float32)
    xin = memory_source_vectors.astype(jnp.float32)
    blocks_in = xin.reshape(SEQ, BLOCKS, BW)
    rec_full = memory_switch_tiles.astype(jnp.float32)
    in_full = entry_switch_tiles.astype(jnp.float32)
    memory_switch_fraction = jax.nn.sigmoid(jnp.einsum('tnc,ncd->tnd', blocks_in, rec_full).reshape(SEQ, D))
    inp_open = jax.nn.sigmoid(jnp.einsum('tnc,ncd->tnd', blocks_in, in_full).reshape(SEQ, D))
    log_fading_factor = -8.0 * memory_switch_fraction * feature_fading_speed[None, :] + extra_log_fading[:, None]
    decay_mult = jnp.exp(log_fading_factor)
    spare_room = -jnp.expm1(2.0 * log_fading_factor)
    in_scale = jnp.sqrt(jnp.maximum(spare_room, 0.01))
    drive = in_scale * inp_open * xin
    coeff = jnp.concatenate([decay_mult[1:], jnp.ones((1, D), jnp.float32)], axis=0)
    _, dstate = lax.associative_scan(compose, (coeff, upstream), reverse=True, axis=0)
    scale_slope = jnp.where(spare_room > 0.01, -decay_mult * decay_mult / in_scale, 0.0)
    log_grad = dstate * (memory_hidden_values.astype(jnp.float32) - drive + scale_slope * inp_open * xin)
    grad_rec = lax.optimization_barrier((log_grad * (-8.0 * feature_fading_speed[None, :]) * memory_switch_fraction * (1.0 - memory_switch_fraction)).astype(jnp.bfloat16)).astype(jnp.float32)
    grad_in = lax.optimization_barrier((dstate * in_scale * xin * inp_open * (1.0 - inp_open)).astype(jnp.bfloat16)).astype(jnp.float32)
    back_rec = jnp.einsum('tnd,ncd->tnc', grad_rec.reshape(SEQ, BLOCKS, BW), rec_full).reshape(SEQ, D)
    back_in = jnp.einsum('tnd,ncd->tnc', grad_in.reshape(SEQ, BLOCKS, BW), in_full).reshape(SEQ, D)
    lru_input_grad = dstate * in_scale * inp_open + back_rec + back_in
    out_proj_grad = jnp.dot(mixed_grad.T, memory_hidden_values, preferred_element_type=jnp.float32)
    gate_proj_grad = gate_grads.reshape(EXPERTS, SLICES, N_TP, D, FE_DEV).transpose(0, 1, 3, 2, 4).reshape(EXPERTS * SLICES, D, N_TP * FE_DEV)
    up_proj_grad = up_grads.reshape(EXPERTS, SLICES, N_TP, D, FE_DEV).transpose(0, 1, 3, 2, 4).reshape(EXPERTS * SLICES, D, N_TP * FE_DEV)
    down_proj_grad = down_grads.reshape(EXPERTS * SLICES, N_TP * FE_DEV, D)
    return (gate_proj_grad, up_proj_grad, down_proj_grad, out_proj_grad, lru_input_grad)
```

```python
import functools

import jax
import jax.numpy as jnp
from jax import lax
from jax.experimental import pallas as pl
from jax.experimental.pallas import tpu as pltpu
from jax.sharding import PartitionSpec as P

SLICES = 2


def prefix(part, axis, combine, identity):
    count = lax.axis_size(axis)
    place = lax.axis_index(axis)
    ahead = count - 1 - place
    gathered = jax.tree.map(lambda a: lax.all_gather(a, axis), part)
    state = jax.tree.map(lambda a, e: jnp.zeros_like(a) + jnp.asarray(e, a.dtype), part, identity)

    def one(turn, state):
        source = count - 1 - turn
        return combine(
            state, jax.tree.map(lambda a: lax.dynamic_index_in_dim(a, source, 0, False), gathered)
        )

    return lax.fori_loop(0, ahead, one, state)


def silu_slope(value):
    sig_value = jax.nn.sigmoid(value)
    return sig_value * (1.0 + value * (1.0 - sig_value))


def compose(upper_map, lower_map):
    return (lower_map[0] * upper_map[0], lower_map[1] + lower_map[0] * upper_map[1])


def chain_join(higher_map, lower_map):
    return (lower_map[0] * higher_map[0], lower_map[1] + lower_map[0] * higher_map[1])


def expert_backward(inputs, grads_in, gate_weight, up_weight, down_weight):
    gate_value = jnp.dot(inputs, gate_weight, preferred_element_type=jnp.float32)
    up_value = jnp.dot(inputs, up_weight, preferred_element_type=jnp.float32)
    active = jax.nn.silu(gate_value)
    hidden = (active * up_value).astype(jnp.bfloat16)
    down_grad = jnp.einsum(
        "rf,rd->fd", hidden, grads_in, preferred_element_type=jnp.float32
    ).astype(jnp.bfloat16)
    hidden_grad = jnp.einsum("rd,fd->rf", grads_in, down_weight, preferred_element_type=jnp.float32)
    gate_grad = (hidden_grad * up_value * silu_slope(gate_value)).astype(jnp.bfloat16)
    up_grad = (hidden_grad * active).astype(jnp.bfloat16)
    gate_weight_grad = jnp.einsum(
        "rd,rf->df", inputs, gate_grad, preferred_element_type=jnp.float32
    ).astype(jnp.bfloat16)
    up_weight_grad = jnp.einsum(
        "rd,rf->df", inputs, up_grad, preferred_element_type=jnp.float32
    ).astype(jnp.bfloat16)
    token_part = jnp.einsum("rf,df->rd", gate_grad, gate_weight, preferred_element_type=jnp.float32)
    token_part = token_part + jnp.einsum(
        "rf,df->rd", up_grad, up_weight, preferred_element_type=jnp.float32
    )
    return (gate_weight_grad, up_weight_grad, down_grad, token_part)


def collect(returned, targets, route_count):
    gathered = jnp.take(returned, targets[0], axis=0).astype(jnp.float32)
    for target in targets[1:]:
        gathered = gathered + jnp.take(returned, target, axis=0).astype(jnp.float32)
    return gathered.reshape(-1, route_count, gathered.shape[-1]).sum(axis=1)


def fill_slots(values, targets, slot_rows):
    buffer = jnp.zeros((slot_rows, values.shape[1]), jnp.bfloat16)
    for target in targets:
        buffer = buffer.at[target].set(values)
    return buffer


MESH_ID = pl.DeviceIdType.MESH


def greet(peers):
    barrier = pltpu.get_barrier_semaphore()
    for peer in peers:
        pl.semaphore_signal(barrier, inc=1, device_id=peer, device_id_type=MESH_ID)
    pl.semaphore_wait(barrier, len(peers))


def remote(src, dst, send, recv, peer):
    return pltpu.make_async_remote_copy(
        src_ref=src, dst_ref=dst, send_sem=send, recv_sem=recv, device_id=peer, device_id_type=MESH_ID
    )


def places(sp_count):
    me = lax.axis_index("sp")
    tp = lax.axis_index("tp")
    side, core = tp // 2, tp % 2
    peers = [(lax.rem(me + k, sp_count), tp) for k in range(sp_count)]
    sources = [lax.rem(me + sp_count - k, sp_count) for k in range(sp_count)]
    sibling = (me, side * 2 + (1 - core))
    across = (me, (1 - side) * 2 + core)
    return me, side, core, peers, sources, sibling, across


def gather_kernel(sp_count, x_ref, g_ref, info_ref, r_ref, h_ref, xo, go, io, ro, ho,
                  ds, dr, ys, yr, ss, sr, s2, r2, local_sem):
    me, side, core, peers, sources, sibling, across = places(sp_count)
    rows, feats = x_ref.shape
    half = feats // 2
    passed = 3 * half // 8
    direct = half - passed
    first = pl.multiple_of(core * half + side * passed, 128)
    onward = pl.multiple_of(core * half + side * direct, 128)
    back = pl.multiple_of(core * half + (1 - side) * direct, 128)

    def at(ref, who, col, width):
        return ref.at[pl.ds(pl.multiple_of(who * rows, rows), rows), pl.ds(col, width)]

    def block(ref, who, size):
        return ref.at[pl.ds(pl.multiple_of(who * size, size), size), :]

    greet(peers[1:] + [sibling, across])
    pairs = ((x_ref, xo), (g_ref, go))
    small = ((info_ref, io), (r_ref, ro), (h_ref, ho))
    waits = []
    copies = {}
    for a, (src, dst) in enumerate(pairs):
        for k in range(1, sp_count):
            cp = remote(src.at[:, pl.ds(first, direct)], at(dst, me, first, direct), ds.at[a, k], dr.at[a, k], peers[k])
            cp.start()
            copies[a, k] = cp
    for b, (src, dst) in enumerate(small):
        for k in range(1, sp_count):
            cp = remote(src, block(dst, me, src.shape[0]), s2.at[b, k], r2.at[b, k], peers[k])
            cp.start()
            waits.append(cp)
    locals_ = []
    for n, (src, dst) in enumerate(pairs + small):
        cp = pltpu.make_async_copy(src, block(dst, me, src.shape[0]), local_sem.at[n])
        cp.start()
        locals_.append(cp)
    for a, (src, dst) in enumerate(pairs):
        for k in range(1, sp_count):
            who = sources[k]
            copies[a, k].wait_recv()
            cp = remote(at(dst, who, onward, passed), at(dst, who, onward, passed), ys.at[a, k], yr.at[a, k], across)
            cp.start()
            copies[a, k, 1] = cp
            cp = remote(at(dst, who, first, direct), at(dst, who, first, direct), ss.at[a, k, 0], sr.at[a, k, 0], sibling)
            cp.start()
            waits.append(cp)
    for a, (src, dst) in enumerate(pairs):
        for k in range(1, sp_count):
            who = sources[k]
            copies[a, k, 1].wait_recv()
            cp = remote(at(dst, who, back, passed), at(dst, who, back, passed), ss.at[a, k, 1], sr.at[a, k, 1], sibling)
            cp.start()
            waits.append(cp)
    for a in range(2):
        for k in range(1, sp_count):
            copies[a, k].wait_send()
            copies[a, k, 1].wait_send()
    for cp in waits + locals_:
        cp.wait()


def gather_all(sp_count, x, g, info, r, h):
    dma = pltpu.SemaphoreType.DMA
    outs = [jax.ShapeDtypeStruct((a.shape[0] * sp_count, a.shape[1]), a.dtype) for a in (x, g, info, r, h)]
    return pl.pallas_call(
        functools.partial(gather_kernel, sp_count),
        out_shape=outs,
        in_specs=[pl.BlockSpec(memory_space=pltpu.VMEM)] * 5,
        out_specs=[pl.BlockSpec(memory_space=pl.ANY)] * 5,
        scratch_shapes=[dma((2, sp_count))] * 4 + [dma((2, sp_count, 2))] * 2 + [dma((3, sp_count))] * 2 + [dma((5,))],
        compiler_params=pltpu.CompilerParams(collective_id=0, has_side_effects=True),
    )(x, g, info, r, h)


def return_kernel(sp_count, p_ref, g_ref, mixed, cols_out, sib, out, got, ybuf, yown,
                  a_s, a_r, b_s, b_r, c_s, c_r, d_s, d_r, local_sem):
    me, side, core, peers, sources, sibling, across = places(sp_count)
    rows, feats = g_ref.shape
    half = feats // 2
    mine = pl.multiple_of(core * half, half)
    theirs = pl.multiple_of((1 - core) * half, half)
    greet(peers[1:] + [sibling, across])
    order = list(range(1, sp_count)) + [0]
    first = {}
    for k in order:
        at = pl.ds(pl.multiple_of(peers[k][0] * rows, rows), rows)
        first[k] = remote(p_ref.at[at, pl.ds(theirs, half)], sib.at[k], a_s.at[k], a_r.at[k], sibling)
        first[k].start()
    second = {}
    for k in order:
        at = pl.ds(pl.multiple_of(peers[k][0] * rows, rows), rows)
        first[k].wait_recv()
        total = p_ref[at, pl.ds(mine, half)].astype(jnp.float32) + sib[k].astype(jnp.float32)
        out[k] = total.astype(jnp.bfloat16)
        if k:
            second[k] = remote(out.at[k], got.at[k], b_s.at[k], b_r.at[k], peers[k])
            second[k].start()
    total = out[0].astype(jnp.float32)
    for k in range(1, sp_count):
        second[k].wait_recv()
        total = total + got[k].astype(jnp.float32)
    yown[...] = total.astype(jnp.bfloat16)
    cross = remote(yown, ybuf, c_s.at[0], c_r.at[0], across)
    cross.start()
    cross.wait()
    part = pl.ds(mine, half)
    total = yown[...].astype(jnp.float32) + ybuf[...].astype(jnp.float32)
    mixed[:, part] = (g_ref[:, part].astype(jnp.float32) + total).astype(jnp.bfloat16)
    share = remote(mixed.at[:, part], mixed.at[:, part], c_s.at[1], c_r.at[1], sibling)
    share.start()
    share.wait()
    width = feats // sp_count
    own = pl.ds(pl.multiple_of(me * rows, rows), rows)
    last = []
    for k in range(1, sp_count):
        cols = pl.ds(pl.multiple_of(peers[k][0] * width, width), width)
        cp = remote(mixed.at[:, cols], cols_out.at[own, :], d_s.at[k], d_r.at[k], peers[k])
        cp.start()
        last.append(cp)
    here = pltpu.make_async_copy(mixed.at[:, pl.ds(pl.multiple_of(me * width, width), width)], cols_out.at[own, :], local_sem)
    here.start()
    here.wait()
    for cp in last:
        cp.wait()
    for k in order:
        first[k].wait_send()
    for k in range(1, sp_count):
        second[k].wait_send()


def return_all(sp_count, partial, g):
    dma = pltpu.SemaphoreType.DMA
    rows, feats = g.shape
    half = feats // 2
    big = pltpu.VMEM((sp_count, rows, half), jnp.bfloat16)
    one = pltpu.VMEM((rows, half), jnp.bfloat16)
    return pl.pallas_call(
        functools.partial(return_kernel, sp_count),
        out_shape=[
            jax.ShapeDtypeStruct((rows, feats), jnp.bfloat16),
            jax.ShapeDtypeStruct((rows * sp_count, feats // sp_count), jnp.bfloat16),
        ],
        in_specs=[pl.BlockSpec(memory_space=pltpu.VMEM)] * 2,
        out_specs=[pl.BlockSpec(memory_space=pltpu.VMEM)] * 2,
        scratch_shapes=[big, big, big, one, one] + [dma((sp_count,))] * 4 + [dma((2,))] * 2 + [dma((sp_count,))] * 2 + [dma],
        compiler_params=pltpu.CompilerParams(collective_id=1, has_side_effects=True),
    )(partial, g)


def carry_kernel(sp_count, c_ref, got, s, r):
    me, side, core, peers, sources, sibling, across = places(sp_count)
    greet(peers[1:])
    copies = []
    for k in range(1, sp_count):
        cp = remote(c_ref, got.at[me], s.at[k], r.at[k], peers[k])
        cp.start()
        copies.append(cp)
    got[me] = c_ref[...]
    for cp in copies:
        cp.wait()


def carry_all(sp_count, block):
    dma = pltpu.SemaphoreType.DMA
    return pl.pallas_call(
        functools.partial(carry_kernel, sp_count),
        out_shape=jax.ShapeDtypeStruct((sp_count,) + block.shape, block.dtype),
        in_specs=[pl.BlockSpec(memory_space=pltpu.VMEM)],
        out_specs=pl.BlockSpec(memory_space=pltpu.VMEM),
        scratch_shapes=[dma((sp_count,))] * 2,
        compiler_params=pltpu.CompilerParams(collective_id=2, has_side_effects=True),
    )(block)


def local(
    result_cotangent_values,
    specialist_entry_vectors,
    chosen_specialists,
    specialist_mixing_shares,
    specialist_switch_maps,
    specialist_widen_maps,
    specialist_shrink_maps,
    memory_readout_map,
    memory_source_vectors,
    memory_hidden_values,
    feature_fading_speed,
    extra_log_fading,
    memory_switch_tiles,
    entry_switch_tiles,
):
    tok_rows, feature_count = result_cotangent_values.shape
    route_count = chosen_specialists.shape[1]
    sp_count = lax.axis_size("sp")
    expert_count = sp_count // SLICES
    capacity = min(tok_rows, 4 * tok_rows // expert_count)
    slot_rows = sp_count * capacity
    flat_expert = chosen_specialists.reshape(-1)
    onehot = (flat_expert[:, None] == jnp.arange(expert_count, dtype=jnp.int32)[None, :]).astype(
        jnp.int32
    )
    slot_rank = jnp.sum((jnp.cumsum(onehot, axis=0) - 1) * onehot, axis=1)
    scaled = (
        (
            specialist_mixing_shares[:, :, None]
            * result_cotangent_values[:, None, :].astype(jnp.float32)
        )
        .astype(jnp.bfloat16)
        .reshape(-1, feature_count)
    )
    copies = jnp.broadcast_to(
        specialist_entry_vectors[:, None, :], (tok_rows, route_count, feature_count)
    ).reshape(-1, feature_count)
    targets = [
        (flat_expert * SLICES + slice_index) * capacity + slot_rank for slice_index in range(SLICES)
    ]
    share = feature_count // lax.axis_size("tp")
    first_col = lax.axis_index("tp") * share
    part_grad = lax.dynamic_slice_in_dim(scaled, first_col, share, 1)
    part_rows = lax.dynamic_slice_in_dim(copies, first_col, share, 1)
    send_grad = fill_slots(part_grad, targets, slot_rows)
    send_rows = fill_slots(part_rows, targets, slot_rows)
    got_grad, got_rows = (
        lax.all_to_all(
            send_grad.reshape(sp_count, capacity, share),
            "sp",
            split_axis=0,
            concat_axis=0,
            tiled=True,
        ),
        lax.all_to_all(
            send_rows.reshape(sp_count, capacity, share),
            "sp",
            split_axis=0,
            concat_axis=0,
            tiled=True,
        ),
    )
    recv_grad, recv_rows = (
        lax.all_gather(got_grad, "tp", axis=2, tiled=True),
        lax.all_gather(got_rows, "tp", axis=2, tiled=True),
    )
    inputs = recv_rows.reshape(slot_rows, feature_count)
    grads_in = recv_grad.reshape(slot_rows, feature_count)
    gate_weight_grad, up_weight_grad, down_grad, token_part = expert_backward(
        inputs,
        grads_in,
        specialist_switch_maps[0],
        specialist_widen_maps[0],
        specialist_shrink_maps[0],
    )
    returned = lax.all_to_all(
        token_part.astype(jnp.bfloat16).reshape(sp_count, capacity, feature_count),
        "sp",
        split_axis=0,
        concat_axis=0,
        tiled=True,
    )
    own_sum = collect(returned.reshape(slot_rows, feature_count), targets, route_count)
    moe_grad = lax.psum(own_sum.astype(jnp.bfloat16), "tp").astype(jnp.float32)
    mixed_grad = (result_cotangent_values.astype(jnp.float32) + moe_grad).astype(jnp.bfloat16)
    col_count = memory_readout_map.shape[1]
    columns = mixed_grad
    upstream = jnp.dot(
        columns,
        lax.all_gather(memory_readout_map, "sp", axis=0, tiled=True),
        preferred_element_type=jnp.float32,
    )
    blocks_here = memory_switch_tiles.shape[0]
    block_width = memory_switch_tiles.shape[1]
    blocks_in = memory_source_vectors.reshape(tok_rows, blocks_here, block_width)
    memory_switch_fraction = jax.nn.sigmoid(
        jnp.einsum(
            "tnc,ncd->tnd", blocks_in, memory_switch_tiles, preferred_element_type=jnp.float32
        ).reshape(tok_rows, col_count)
    )
    inp_open = jax.nn.sigmoid(
        jnp.einsum(
            "tnc,ncd->tnd", blocks_in, entry_switch_tiles, preferred_element_type=jnp.float32
        ).reshape(tok_rows, col_count)
    )
    xin = memory_source_vectors.astype(jnp.float32)
    log_fading_factor = (
        -8.0 * memory_switch_fraction * feature_fading_speed[None, :] + extra_log_fading[:, None]
    )
    decay_mult = jnp.exp(log_fading_factor)
    spare_room = -jnp.expm1(2.0 * log_fading_factor)
    in_scale = jnp.sqrt(jnp.maximum(spare_room, 0.01))
    drive = in_scale * inp_open * xin
    coeff = jnp.concatenate([decay_mult[1:], jnp.ones((1, col_count), jnp.float32)], axis=0)
    prod_after, local_part = lax.associative_scan(compose, (coeff, upstream), reverse=True, axis=0)
    alpha_part = decay_mult[0] * local_part[0]
    beta_part = decay_mult[0] * prod_after[0]
    carried = prefix(
        (beta_part, alpha_part),
        "sp",
        chain_join,
        (jnp.ones_like(beta_part), jnp.zeros_like(alpha_part)),
    )
    incoming = carried[1]
    dstate = local_part + prod_after * incoming[None, :]
    scale_slope = jnp.where(spare_room > 0.01, -decay_mult * decay_mult / in_scale, 0.0)
    log_grad = dstate * (
        memory_hidden_values.astype(jnp.float32) - drive + scale_slope * inp_open * xin
    )
    grad_rec = (
        log_grad
        * (-8.0 * feature_fading_speed[None, :])
        * memory_switch_fraction
        * (1.0 - memory_switch_fraction)
    ).astype(jnp.bfloat16)
    grad_in = (dstate * in_scale * xin * inp_open * (1.0 - inp_open)).astype(jnp.bfloat16)
    back_rec = jnp.einsum(
        "tnd,ncd->tnc",
        grad_rec.reshape(tok_rows, blocks_here, block_width),
        memory_switch_tiles,
        preferred_element_type=jnp.float32,
    )
    back_in = jnp.einsum(
        "tnd,ncd->tnc",
        grad_in.reshape(tok_rows, blocks_here, block_width),
        entry_switch_tiles,
        preferred_element_type=jnp.float32,
    )
    lru_input_grad = (
        dstate * in_scale * inp_open
        + back_rec.reshape(tok_rows, col_count)
        + back_in.reshape(tok_rows, col_count)
    )
    columns = mixed_grad
    out_proj_grad = lax.psum_scatter(
        jnp.einsum("tr,tc->rc", columns, memory_hidden_values, preferred_element_type=jnp.float32),
        "sp",
        scatter_dimension=0,
        tiled=True,
    )
    return (
        gate_weight_grad[None],
        up_weight_grad[None],
        down_grad[None],
        out_proj_grad,
        lru_input_grad,
    )


def direct(
    result_cotangent_values,
    specialist_entry_vectors,
    chosen_specialists,
    specialist_mixing_shares,
    specialist_switch_maps,
    specialist_widen_maps,
    specialist_shrink_maps,
    memory_readout_map,
    memory_source_vectors,
    memory_hidden_values,
    feature_fading_speed,
    extra_log_fading,
    memory_switch_tiles,
    entry_switch_tiles,
):
    tok_rows, feature_count = result_cotangent_values.shape
    sp_count = lax.axis_size("sp")
    info = jnp.concatenate(
        [
            chosen_specialists.astype(jnp.float32).T,
            specialist_mixing_shares.T,
            jnp.zeros((4, tok_rows), jnp.float32),
        ],
        axis=0,
    )
    inputs, all_grad, info, readout, hidden_all = gather_all(
        sp_count,
        specialist_entry_vectors,
        result_cotangent_values,
        info,
        memory_readout_map,
        memory_hidden_values,
    )
    expert = (lax.axis_index("sp") // SLICES).astype(jnp.float32)
    info = info.reshape(sp_count, 8, tok_rows)
    share = jnp.where(info[:, 0] == expert, info[:, 2], 0.0) + jnp.where(
        info[:, 1] == expert, info[:, 3], 0.0
    )
    grads_in = (share.reshape(-1, 1) * all_grad.astype(jnp.float32)).astype(jnp.bfloat16)
    gate_weight_grad, up_weight_grad, down_grad, token_part = expert_backward(
        inputs,
        grads_in,
        specialist_switch_maps[0],
        specialist_widen_maps[0],
        specialist_shrink_maps[0],
    )
    mixed_grad, mixed_cols = return_all(
        sp_count, token_part.astype(jnp.bfloat16), result_cotangent_values
    )
    col_count = memory_readout_map.shape[1]
    upstream = jnp.dot(mixed_grad, readout, preferred_element_type=jnp.float32)
    blocks_here = memory_switch_tiles.shape[0]
    block_width = memory_switch_tiles.shape[1]
    blocks_in = memory_source_vectors.reshape(tok_rows, blocks_here, block_width)
    memory_switch_fraction = jax.nn.sigmoid(
        jnp.einsum(
            "tnc,ncd->tnd", blocks_in, memory_switch_tiles, preferred_element_type=jnp.float32
        ).reshape(tok_rows, col_count)
    )
    inp_open = jax.nn.sigmoid(
        jnp.einsum(
            "tnc,ncd->tnd", blocks_in, entry_switch_tiles, preferred_element_type=jnp.float32
        ).reshape(tok_rows, col_count)
    )
    xin = memory_source_vectors.astype(jnp.float32)
    log_fading_factor = (
        -8.0 * memory_switch_fraction * feature_fading_speed[None, :] + extra_log_fading[:, None]
    )
    decay_mult = jnp.exp(log_fading_factor)
    spare_room = -jnp.expm1(2.0 * log_fading_factor)
    in_scale = jnp.sqrt(jnp.maximum(spare_room, 0.01))
    drive = in_scale * inp_open * xin
    coeff = jnp.concatenate([decay_mult[1:], jnp.ones((1, col_count), jnp.float32)], axis=0)
    prod_after, local_part = lax.associative_scan(compose, (coeff, upstream), reverse=True, axis=0)
    alpha_part = decay_mult[0] * local_part[0]
    beta_part = decay_mult[0] * prod_after[0]
    gathered = carry_all(
        sp_count,
        jnp.concatenate(
            [beta_part[None], alpha_part[None], jnp.zeros((6, col_count), jnp.float32)], axis=0
        ),
    )
    place = lax.axis_index("sp")
    incoming = jnp.zeros((col_count,), jnp.float32)
    for source in range(sp_count - 1, 0, -1):
        incoming = jnp.where(
            source > place, gathered[source, 1] + gathered[source, 0] * incoming, incoming
        )
    dstate = local_part + prod_after * incoming[None, :]
    scale_slope = jnp.where(spare_room > 0.01, -decay_mult * decay_mult / in_scale, 0.0)
    log_grad = dstate * (
        memory_hidden_values.astype(jnp.float32) - drive + scale_slope * inp_open * xin
    )
    grad_rec = (
        log_grad
        * (-8.0 * feature_fading_speed[None, :])
        * memory_switch_fraction
        * (1.0 - memory_switch_fraction)
    ).astype(jnp.bfloat16)
    grad_in = (dstate * in_scale * xin * inp_open * (1.0 - inp_open)).astype(jnp.bfloat16)
    back_rec = jnp.einsum(
        "tnd,ncd->tnc",
        grad_rec.reshape(tok_rows, blocks_here, block_width),
        memory_switch_tiles,
        preferred_element_type=jnp.float32,
    )
    back_in = jnp.einsum(
        "tnd,ncd->tnc",
        grad_in.reshape(tok_rows, blocks_here, block_width),
        entry_switch_tiles,
        preferred_element_type=jnp.float32,
    )
    lru_input_grad = (
        dstate * in_scale * inp_open
        + back_rec.reshape(tok_rows, col_count)
        + back_in.reshape(tok_rows, col_count)
    )
    out_proj_grad = jnp.einsum(
        "tr,tc->rc", mixed_cols, hidden_all, preferred_element_type=jnp.float32
    )
    return (
        gate_weight_grad[None],
        up_weight_grad[None],
        down_grad[None],
        out_proj_grad,
        lru_input_grad,
    )


def solution(mesh):
    sp_count, tp_count = mesh.shape["sp"], mesh.shape["tp"]
    whole_blocks = 4 * SLICES == sp_count and tp_count == 4
    return jax.shard_map(
        direct if whole_blocks else local,
        mesh=mesh,
        in_specs=(
            P("sp", None),
            P("sp", None),
            P("sp", None),
            P("sp", None),
            P("sp", None, "tp"),
            P("sp", None, "tp"),
            P("sp", "tp", None),
            P("sp", "tp"),
            P("sp", "tp"),
            P("sp", "tp"),
            P("tp"),
            P("sp"),
            P("tp", None, None),
            P("tp", None, None),
        ),
        out_specs=(
            P("sp", None, "tp"),
            P("sp", None, "tp"),
            P("sp", "tp", None),
            P("sp", "tp"),
            P("sp", "tp"),
        ),
        check_vma=False,
    )
```

```python
import functools

import jax
import jax.numpy as jnp
from jax import lax
from jax.experimental import pallas as pl
from jax.experimental.pallas import tpu as pltpu
from jax.sharding import PartitionSpec as P

SLICES = 2


def prefix(part, axis, combine, identity):
    count = lax.axis_size(axis)
    place = lax.axis_index(axis)
    ahead = count - 1 - place
    gathered = jax.tree.map(lambda a: lax.all_gather(a, axis), part)
    state = jax.tree.map(lambda a, e: jnp.zeros_like(a) + jnp.asarray(e, a.dtype), part, identity)

    def one(turn, state):
        source = count - 1 - turn
        return combine(
            state, jax.tree.map(lambda a: lax.dynamic_index_in_dim(a, source, 0, False), gathered)
        )

    return lax.fori_loop(0, ahead, one, state)


def silu_slope(value):
    sig_value = jax.nn.sigmoid(value)
    return sig_value * (1.0 + value * (1.0 - sig_value))


def compose(upper_map, lower_map):
    return (lower_map[0] * upper_map[0], lower_map[1] + lower_map[0] * upper_map[1])


def chain_join(higher_map, lower_map):
    return (lower_map[0] * higher_map[0], lower_map[1] + lower_map[0] * higher_map[1])


def expert_backward(inputs, grads_in, gate_weight, up_weight, down_weight):
    gate_value = jnp.dot(inputs, gate_weight, preferred_element_type=jnp.float32)
    up_value = jnp.dot(inputs, up_weight, preferred_element_type=jnp.float32)
    active = jax.nn.silu(gate_value)
    hidden = (active * up_value).astype(jnp.bfloat16)
    down_grad = jnp.einsum(
        "rf,rd->fd", hidden, grads_in, preferred_element_type=jnp.float32
    ).astype(jnp.bfloat16)
    hidden_grad = jnp.einsum("rd,fd->rf", grads_in, down_weight, preferred_element_type=jnp.float32)
    gate_grad = (hidden_grad * up_value * silu_slope(gate_value)).astype(jnp.bfloat16)
    up_grad = (hidden_grad * active).astype(jnp.bfloat16)
    gate_weight_grad = jnp.einsum(
        "rd,rf->df", inputs, gate_grad, preferred_element_type=jnp.float32
    ).astype(jnp.bfloat16)
    up_weight_grad = jnp.einsum(
        "rd,rf->df", inputs, up_grad, preferred_element_type=jnp.float32
    ).astype(jnp.bfloat16)
    token_part = jnp.einsum("rf,df->rd", gate_grad, gate_weight, preferred_element_type=jnp.float32)
    token_part = token_part + jnp.einsum(
        "rf,df->rd", up_grad, up_weight, preferred_element_type=jnp.float32
    )
    return (gate_weight_grad, up_weight_grad, down_grad, token_part)


def collect(returned, targets, route_count):
    gathered = jnp.take(returned, targets[0], axis=0).astype(jnp.float32)
    for target in targets[1:]:
        gathered = gathered + jnp.take(returned, target, axis=0).astype(jnp.float32)
    return gathered.reshape(-1, route_count, gathered.shape[-1]).sum(axis=1)


def fill_slots(values, targets, slot_rows):
    buffer = jnp.zeros((slot_rows, values.shape[1]), jnp.bfloat16)
    for target in targets:
        buffer = buffer.at[target].set(values)
    return buffer


MESH_ID = pl.DeviceIdType.MESH


def greet(peers):
    barrier = pltpu.get_barrier_semaphore()
    for peer in peers:
        pl.semaphore_signal(barrier, inc=1, device_id=peer, device_id_type=MESH_ID)
    pl.semaphore_wait(barrier, len(peers))


def remote(src, dst, send, recv, peer):
    return pltpu.make_async_remote_copy(
        src_ref=src, dst_ref=dst, send_sem=send, recv_sem=recv, device_id=peer, device_id_type=MESH_ID
    )


def places(sp_count):
    me = lax.axis_index("sp")
    tp = lax.axis_index("tp")
    side, core = tp // 2, tp % 2
    peers = [(lax.rem(me + k, sp_count), tp) for k in range(sp_count)]
    sources = [lax.rem(me + sp_count - k, sp_count) for k in range(sp_count)]
    sibling = (me, side * 2 + (1 - core))
    across = (me, (1 - side) * 2 + core)
    return me, side, core, peers, sources, sibling, across


def gather_kernel(sp_count, x_ref, g_ref, info_ref, r_ref, h_ref, xo, go, io, ro, ho,
                  zs, zr, xs, xr, ys, yr, ss, sr, ts, tr, local_sem):
    me, side, core, peers, sources, sibling, across = places(sp_count)
    tp = lax.axis_index("tp")
    rows, feats = x_ref.shape
    half = feats // 2
    passed = 3 * half // 8
    direct = half - passed
    first = pl.multiple_of(core * half + side * passed, 128)
    onward = pl.multiple_of(core * half + side * direct, 128)
    back = pl.multiple_of(core * half + (1 - side) * direct, 128)
    depth = sp_count // 2
    z, x = me // 2, me % 2
    partner = (z * 2 + 1 - x, tp)
    along = [(lax.rem(z + k, depth) * 2 + x, tp) for k in range(depth)]
    line = [lax.rem(z + depth - k, depth) * 2 for k in range(depth)]

    def at(ref, who, col, width):
        return ref.at[pl.ds(pl.multiple_of(who * rows, rows), rows), pl.ds(col, width)]

    def block(ref, who, size):
        return ref.at[pl.ds(pl.multiple_of(who * size, size), size), :]

    greet(along[1:] + [partner, sibling, across])
    pairs = ((x_ref, xo), (g_ref, go))
    small = ((info_ref, io), (r_ref, ro), (h_ref, ho))
    waits = []
    recv = {}

    def send(key, src, dst, sems, index, peer):
        cp = remote(src, dst, sems[0].at[index], sems[1].at[index], peer)
        cp.start()
        recv[key] = cp

    for n, (src, dst) in enumerate(pairs + small):
        cp = pltpu.make_async_copy(src, block(dst, me, src.shape[0]), local_sem.at[n])
        cp.start()
        waits.append(cp)

    def open_pair(a):
        src, dst = pairs[a]
        for k in range(depth - 1, 0, -1):
            send(("z", a, k), src.at[:, pl.ds(first, direct)], at(dst, me, first, direct), (zs, zr), (a, k), along[k])
        send(("x", a, 0), src.at[:, pl.ds(first, direct)], at(dst, me, first, direct), (xs, xr), (a, 0), partner)

    def spread(a, who, n):
        dst = pairs[a][1]
        send(("y", a, n), at(dst, who, onward, passed), at(dst, who, onward, passed), (ys, yr), (a, n), across)
        send(("s", a, n), at(dst, who, first, direct), at(dst, who, first, direct), (ss, sr), (a, n), sibling)

    def open_small(b):
        src, dst = small[b]
        size = src.shape[0]
        for k in range(depth - 1, 0, -1):
            send(("z", 2 + b, k), src, block(dst, me, size), (zs, zr), (2 + b, k), along[k])
        send(("x", 2 + b, 0), src, block(dst, me, size), (xs, xr), (2 + b, 0), partner)

    open_pair(0)
    open_small(0)
    open_pair(1)
    for a in range(2):
        for k in range(1, depth):
            recv["z", a, k].wait_recv()
            who = line[k] + x
            dst = pairs[a][1]
            send(("x", a, k), at(dst, who, first, direct), at(dst, who, first, direct), (xs, xr), (a, k), partner)
            spread(a, who, k)
        if a == 1:
            open_small(1)
            open_small(2)
        for k in range(depth):
            recv["x", a, k].wait_recv()
            spread(a, line[k] + 1 - x, depth + k)
    for b in range(3):
        dst = small[b][1]
        size = small[b][0].shape[0]
        for k in range(1, depth):
            recv["z", 2 + b, k].wait_recv()
            who = line[k] + x
            send(("x", 2 + b, k), block(dst, who, size), block(dst, who, size), (xs, xr), (2 + b, k), partner)
    for a in range(2):
        dst = pairs[a][1]
        for n in range(1, 2 * depth):
            recv["y", a, n].wait_recv()
            who = line[n] + x if n < depth else line[n - depth] + 1 - x
            send(("t", a, n), at(dst, who, back, passed), at(dst, who, back, passed), (ts, tr), (a, n), sibling)
    for b in range(3):
        for k in range(depth):
            recv["x", 2 + b, k].wait_recv()
    for a in range(2):
        for n in range(1, 2 * depth):
            recv["s", a, n].wait_recv()
            recv["t", a, n].wait_recv()
    for cp in recv.values():
        cp.wait_send()
    for cp in waits:
        cp.wait()


def gather_all(sp_count, x, g, info, r, h):
    dma = pltpu.SemaphoreType.DMA
    outs = [jax.ShapeDtypeStruct((a.shape[0] * sp_count, a.shape[1]), a.dtype) for a in (x, g, info, r, h)]
    return pl.pallas_call(
        functools.partial(gather_kernel, sp_count),
        out_shape=outs,
        in_specs=[pl.BlockSpec(memory_space=pltpu.VMEM)] * 5,
        out_specs=[pl.BlockSpec(memory_space=pl.ANY)] * 5,
        scratch_shapes=[dma((5, sp_count))] * 4 + [dma((2, sp_count))] * 6 + [dma((5,))],
        compiler_params=pltpu.CompilerParams(collective_id=0, has_side_effects=True),
    )(x, g, info, r, h)


def return_kernel(sp_count, p_ref, g_ref, mixed, sib, out, ygot, last, got,
                  a_s, a_r, y_s, y_r, b_s, b_r, c_s, c_r):
    me, side, core, peers, sources, sibling, across = places(sp_count)
    rows, feats = g_ref.shape
    half, quarter = feats // 2, feats // 4
    mine = pl.multiple_of(core * half, half)
    theirs = pl.multiple_of((1 - core) * half, half)
    own = pl.ds(pl.multiple_of(side * quarter, quarter), quarter)
    other = pl.ds(pl.multiple_of((1 - side) * quarter, quarter), quarter)
    greet(peers[1:] + [sibling, across])
    order = list(range(sp_count // 2, 0, -1)) + list(range(sp_count // 2 + 1, sp_count)) + [0]
    first, second, third = {}, {}, {}
    for k in order:
        at = pl.ds(pl.multiple_of(peers[k][0] * rows, rows), rows)
        first[k] = remote(p_ref.at[at, pl.ds(theirs, half)], sib.at[k], a_s.at[k], a_r.at[k], sibling)
        first[k].start()
    for k in order:
        at = pl.ds(pl.multiple_of(peers[k][0] * rows, rows), rows)
        first[k].wait_recv()
        total = p_ref[at, pl.ds(mine, half)].astype(jnp.float32) + sib[k].astype(jnp.float32)
        out[k] = total.astype(jnp.bfloat16)
        second[k] = remote(out.at[k, :, other], ygot.at[k], y_s.at[k], y_r.at[k], across)
        second[k].start()
    for k in order:
        second[k].wait_recv()
        total = out[k, :, own].astype(jnp.float32) + ygot[k].astype(jnp.float32)
        last[k] = total.astype(jnp.bfloat16)
        if k:
            third[k] = remote(last.at[k], got.at[k], b_s.at[k], b_r.at[k], peers[k])
            third[k].start()
    total = last[0].astype(jnp.float32)
    for k in order[:-1]:
        third[k].wait_recv()
        total = total + got[k].astype(jnp.float32)
    here = pl.ds(pl.multiple_of(core * half + side * quarter, quarter), quarter)
    there = pl.ds(pl.multiple_of(core * half + (1 - side) * quarter, quarter), quarter)
    mixed[:, here] = (g_ref[:, here].astype(jnp.float32) + total).astype(jnp.bfloat16)
    ends = []
    for n, (cols, who) in enumerate(((here, across), (here, sibling), (there, sibling))):
        if n == 2:
            ends[0].wait_recv()
        cp = remote(mixed.at[:, cols], mixed.at[:, cols], c_s.at[n], c_r.at[n], who)
        cp.start()
        ends.append(cp)
    ends[1].wait_recv()
    ends[2].wait_recv()
    for cp in ends + list(first.values()) + list(second.values()) + list(third.values()):
        cp.wait_send()


def return_all(sp_count, partial, g):
    dma = pltpu.SemaphoreType.DMA
    rows, feats = g.shape
    big = pltpu.VMEM((sp_count, rows, feats // 2), jnp.bfloat16)
    small = pltpu.VMEM((sp_count, rows, feats // 4), jnp.bfloat16)
    return pl.pallas_call(
        functools.partial(return_kernel, sp_count),
        out_shape=jax.ShapeDtypeStruct((rows, feats), jnp.bfloat16),
        in_specs=[pl.BlockSpec(memory_space=pltpu.VMEM)] * 2,
        out_specs=pl.BlockSpec(memory_space=pltpu.VMEM),
        scratch_shapes=[big, big, small, small, small] + [dma((sp_count,))] * 6 + [dma((3,))] * 2,
        compiler_params=pltpu.CompilerParams(collective_id=1, has_side_effects=True),
    )(partial, g)


def carry_kernel(sp_count, mixed, decay_ref, up_ref, dstate, cols_out, block, got, s, r, d_s, d_r, local_sem):
    me, side, core, peers, sources, sibling, across = places(sp_count)
    rows, feats = mixed.shape
    width = feats // sp_count
    greet(peers[1:])
    own = pl.ds(pl.multiple_of(me * rows, rows), rows)
    moved = []
    for k in range(1, sp_count):
        cols = pl.ds(pl.multiple_of(peers[k][0] * width, width), width)
        cp = remote(mixed.at[:, cols], cols_out.at[own, :], d_s.at[k], d_r.at[k], peers[k])
        cp.start()
        moved.append(cp)
    here = pltpu.make_async_copy(
        mixed.at[:, pl.ds(pl.multiple_of(me * width, width), width)], cols_out.at[own, :], local_sem
    )
    here.start()
    row = lax.broadcasted_iota(jnp.int32, up_ref.shape, 0)
    decay = decay_ref[...]
    prod = jnp.where(row < rows - 1, pltpu.roll(decay, rows - 1, 0), 1.0)
    part = up_ref[...]
    step = 1
    while step < rows:
        keep = row < rows - step
        later = jnp.where(keep, pltpu.roll(part, rows - step, 0), 0.0)
        after = jnp.where(keep, pltpu.roll(prod, rows - step, 0), 1.0)
        part = part + prod * later
        prod = prod * after
        step *= 2
    block[...] = jnp.zeros_like(block)
    got[me] = jnp.zeros(block.shape, jnp.float32)
    block[0:1] = decay[0:1] * prod[0:1]
    block[1:2] = decay[0:1] * part[0:1]
    copies = []
    for k in range(1, sp_count):
        cp = remote(block, got.at[me], s.at[k], r.at[k], peers[k])
        cp.start()
        copies.append(cp)
    for cp in copies:
        cp.wait()
    incoming = jnp.zeros((1, up_ref.shape[1]), jnp.float32)
    for source in range(sp_count - 1, 0, -1):
        value = got[source]
        incoming = jnp.where(source > me, value[1:2] + value[0:1] * incoming, incoming)
    dstate[...] = part + prod * incoming
    here.wait()
    for cp in moved:
        cp.wait()


def carry_all(sp_count, mixed, decay, upstream):
    dma = pltpu.SemaphoreType.DMA
    rows, feats = mixed.shape
    block = (8, upstream.shape[1])
    return pl.pallas_call(
        functools.partial(carry_kernel, sp_count),
        out_shape=[
            jax.ShapeDtypeStruct(upstream.shape, jnp.float32),
            jax.ShapeDtypeStruct((rows * sp_count, feats // sp_count), jnp.bfloat16),
        ],
        in_specs=[pl.BlockSpec(memory_space=pltpu.VMEM)] * 3,
        out_specs=[pl.BlockSpec(memory_space=pltpu.VMEM)] * 2,
        scratch_shapes=[pltpu.VMEM(block, jnp.float32), pltpu.VMEM((sp_count,) + block, jnp.float32)]
        + [dma((sp_count,))] * 4
        + [dma],
        compiler_params=pltpu.CompilerParams(collective_id=2, has_side_effects=True),
    )(mixed, decay, upstream)


def local(
    result_cotangent_values,
    specialist_entry_vectors,
    chosen_specialists,
    specialist_mixing_shares,
    specialist_switch_maps,
    specialist_widen_maps,
    specialist_shrink_maps,
    memory_readout_map,
    memory_source_vectors,
    memory_hidden_values,
    feature_fading_speed,
    extra_log_fading,
    memory_switch_tiles,
    entry_switch_tiles,
):
    tok_rows, feature_count = result_cotangent_values.shape
    route_count = chosen_specialists.shape[1]
    sp_count = lax.axis_size("sp")
    expert_count = sp_count // SLICES
    capacity = min(tok_rows, 4 * tok_rows // expert_count)
    slot_rows = sp_count * capacity
    flat_expert = chosen_specialists.reshape(-1)
    onehot = (flat_expert[:, None] == jnp.arange(expert_count, dtype=jnp.int32)[None, :]).astype(
        jnp.int32
    )
    slot_rank = jnp.sum((jnp.cumsum(onehot, axis=0) - 1) * onehot, axis=1)
    scaled = (
        (
            specialist_mixing_shares[:, :, None]
            * result_cotangent_values[:, None, :].astype(jnp.float32)
        )
        .astype(jnp.bfloat16)
        .reshape(-1, feature_count)
    )
    copies = jnp.broadcast_to(
        specialist_entry_vectors[:, None, :], (tok_rows, route_count, feature_count)
    ).reshape(-1, feature_count)
    targets = [
        (flat_expert * SLICES + slice_index) * capacity + slot_rank for slice_index in range(SLICES)
    ]
    share = feature_count // lax.axis_size("tp")
    first_col = lax.axis_index("tp") * share
    part_grad = lax.dynamic_slice_in_dim(scaled, first_col, share, 1)
    part_rows = lax.dynamic_slice_in_dim(copies, first_col, share, 1)
    send_grad = fill_slots(part_grad, targets, slot_rows)
    send_rows = fill_slots(part_rows, targets, slot_rows)
    got_grad, got_rows = (
        lax.all_to_all(
            send_grad.reshape(sp_count, capacity, share),
            "sp",
            split_axis=0,
            concat_axis=0,
            tiled=True,
        ),
        lax.all_to_all(
            send_rows.reshape(sp_count, capacity, share),
            "sp",
            split_axis=0,
            concat_axis=0,
            tiled=True,
        ),
    )
    recv_grad, recv_rows = (
        lax.all_gather(got_grad, "tp", axis=2, tiled=True),
        lax.all_gather(got_rows, "tp", axis=2, tiled=True),
    )
    inputs = recv_rows.reshape(slot_rows, feature_count)
    grads_in = recv_grad.reshape(slot_rows, feature_count)
    gate_weight_grad, up_weight_grad, down_grad, token_part = expert_backward(
        inputs,
        grads_in,
        specialist_switch_maps[0],
        specialist_widen_maps[0],
        specialist_shrink_maps[0],
    )
    returned = lax.all_to_all(
        token_part.astype(jnp.bfloat16).reshape(sp_count, capacity, feature_count),
        "sp",
        split_axis=0,
        concat_axis=0,
        tiled=True,
    )
    own_sum = collect(returned.reshape(slot_rows, feature_count), targets, route_count)
    moe_grad = lax.psum(own_sum.astype(jnp.bfloat16), "tp").astype(jnp.float32)
    mixed_grad = (result_cotangent_values.astype(jnp.float32) + moe_grad).astype(jnp.bfloat16)
    col_count = memory_readout_map.shape[1]
    columns = mixed_grad
    upstream = jnp.dot(
        columns,
        lax.all_gather(memory_readout_map, "sp", axis=0, tiled=True),
        preferred_element_type=jnp.float32,
    )
    blocks_here = memory_switch_tiles.shape[0]
    block_width = memory_switch_tiles.shape[1]
    blocks_in = memory_source_vectors.reshape(tok_rows, blocks_here, block_width)
    memory_switch_fraction = jax.nn.sigmoid(
        jnp.einsum(
            "tnc,ncd->tnd", blocks_in, memory_switch_tiles, preferred_element_type=jnp.float32
        ).reshape(tok_rows, col_count)
    )
    inp_open = jax.nn.sigmoid(
        jnp.einsum(
            "tnc,ncd->tnd", blocks_in, entry_switch_tiles, preferred_element_type=jnp.float32
        ).reshape(tok_rows, col_count)
    )
    xin = memory_source_vectors.astype(jnp.float32)
    log_fading_factor = (
        -8.0 * memory_switch_fraction * feature_fading_speed[None, :] + extra_log_fading[:, None]
    )
    decay_mult = jnp.exp(log_fading_factor)
    spare_room = -jnp.expm1(2.0 * log_fading_factor)
    in_scale = jnp.sqrt(jnp.maximum(spare_room, 0.01))
    drive = in_scale * inp_open * xin
    coeff = jnp.concatenate([decay_mult[1:], jnp.ones((1, col_count), jnp.float32)], axis=0)
    prod_after, local_part = lax.associative_scan(compose, (coeff, upstream), reverse=True, axis=0)
    alpha_part = decay_mult[0] * local_part[0]
    beta_part = decay_mult[0] * prod_after[0]
    carried = prefix(
        (beta_part, alpha_part),
        "sp",
        chain_join,
        (jnp.ones_like(beta_part), jnp.zeros_like(alpha_part)),
    )
    incoming = carried[1]
    dstate = local_part + prod_after * incoming[None, :]
    scale_slope = jnp.where(spare_room > 0.01, -decay_mult * decay_mult / in_scale, 0.0)
    log_grad = dstate * (
        memory_hidden_values.astype(jnp.float32) - drive + scale_slope * inp_open * xin
    )
    grad_rec = (
        log_grad
        * (-8.0 * feature_fading_speed[None, :])
        * memory_switch_fraction
        * (1.0 - memory_switch_fraction)
    ).astype(jnp.bfloat16)
    grad_in = (dstate * in_scale * xin * inp_open * (1.0 - inp_open)).astype(jnp.bfloat16)
    back_rec = jnp.einsum(
        "tnd,ncd->tnc",
        grad_rec.reshape(tok_rows, blocks_here, block_width),
        memory_switch_tiles,
        preferred_element_type=jnp.float32,
    )
    back_in = jnp.einsum(
        "tnd,ncd->tnc",
        grad_in.reshape(tok_rows, blocks_here, block_width),
        entry_switch_tiles,
        preferred_element_type=jnp.float32,
    )
    lru_input_grad = (
        dstate * in_scale * inp_open
        + back_rec.reshape(tok_rows, col_count)
        + back_in.reshape(tok_rows, col_count)
    )
    columns = mixed_grad
    out_proj_grad = lax.psum_scatter(
        jnp.einsum("tr,tc->rc", columns, memory_hidden_values, preferred_element_type=jnp.float32),
        "sp",
        scatter_dimension=0,
        tiled=True,
    )
    return (
        gate_weight_grad[None],
        up_weight_grad[None],
        down_grad[None],
        out_proj_grad,
        lru_input_grad,
    )


def direct(
    result_cotangent_values,
    specialist_entry_vectors,
    chosen_specialists,
    specialist_mixing_shares,
    specialist_switch_maps,
    specialist_widen_maps,
    specialist_shrink_maps,
    memory_readout_map,
    memory_source_vectors,
    memory_hidden_values,
    feature_fading_speed,
    extra_log_fading,
    memory_switch_tiles,
    entry_switch_tiles,
):
    tok_rows, feature_count = result_cotangent_values.shape
    sp_count = lax.axis_size("sp")
    info = jnp.concatenate(
        [
            chosen_specialists.astype(jnp.float32).T,
            specialist_mixing_shares.T,
            jnp.zeros((4, tok_rows), jnp.float32),
        ],
        axis=0,
    )
    inputs, all_grad, info, readout, hidden_all = gather_all(
        sp_count,
        specialist_entry_vectors,
        result_cotangent_values,
        info,
        memory_readout_map,
        memory_hidden_values,
    )
    expert = (lax.axis_index("sp") // SLICES).astype(jnp.float32)
    info = info.reshape(sp_count, 8, tok_rows)
    share = jnp.where(info[:, 0] == expert, info[:, 2], 0.0) + jnp.where(
        info[:, 1] == expert, info[:, 3], 0.0
    )
    grads_in = (share.reshape(-1, 1) * all_grad.astype(jnp.float32)).astype(jnp.bfloat16)
    gate_weight_grad, up_weight_grad, down_grad, token_part = expert_backward(
        inputs,
        grads_in,
        specialist_switch_maps[0],
        specialist_widen_maps[0],
        specialist_shrink_maps[0],
    )
    mixed_grad = return_all(
        sp_count, token_part.astype(jnp.bfloat16), result_cotangent_values
    )
    col_count = memory_readout_map.shape[1]
    upstream = jnp.dot(mixed_grad, readout, preferred_element_type=jnp.float32)
    blocks_here = memory_switch_tiles.shape[0]
    block_width = memory_switch_tiles.shape[1]
    blocks_in = memory_source_vectors.reshape(tok_rows, blocks_here, block_width)
    memory_switch_fraction = jax.nn.sigmoid(
        jnp.einsum(
            "tnc,ncd->tnd", blocks_in, memory_switch_tiles, preferred_element_type=jnp.float32
        ).reshape(tok_rows, col_count)
    )
    inp_open = jax.nn.sigmoid(
        jnp.einsum(
            "tnc,ncd->tnd", blocks_in, entry_switch_tiles, preferred_element_type=jnp.float32
        ).reshape(tok_rows, col_count)
    )
    xin = memory_source_vectors.astype(jnp.float32)
    log_fading_factor = (
        -8.0 * memory_switch_fraction * feature_fading_speed[None, :] + extra_log_fading[:, None]
    )
    decay_mult = jnp.exp(log_fading_factor)
    spare_room = -jnp.expm1(2.0 * log_fading_factor)
    in_scale = jnp.sqrt(jnp.maximum(spare_room, 0.01))
    drive = in_scale * inp_open * xin
    dstate, mixed_cols = carry_all(sp_count, mixed_grad, decay_mult, upstream)
    scale_slope = jnp.where(spare_room > 0.01, -decay_mult * decay_mult / in_scale, 0.0)
    log_grad = dstate * (
        memory_hidden_values.astype(jnp.float32) - drive + scale_slope * inp_open * xin
    )
    grad_rec = (
        log_grad
        * (-8.0 * feature_fading_speed[None, :])
        * memory_switch_fraction
        * (1.0 - memory_switch_fraction)
    ).astype(jnp.bfloat16)
    grad_in = (dstate * in_scale * xin * inp_open * (1.0 - inp_open)).astype(jnp.bfloat16)
    back_rec = jnp.einsum(
        "tnd,ncd->tnc",
        grad_rec.reshape(tok_rows, blocks_here, block_width),
        memory_switch_tiles,
        preferred_element_type=jnp.float32,
    )
    back_in = jnp.einsum(
        "tnd,ncd->tnc",
        grad_in.reshape(tok_rows, blocks_here, block_width),
        entry_switch_tiles,
        preferred_element_type=jnp.float32,
    )
    lru_input_grad = (
        dstate * in_scale * inp_open
        + back_rec.reshape(tok_rows, col_count)
        + back_in.reshape(tok_rows, col_count)
    )
    out_proj_grad = jnp.einsum(
        "tr,tc->rc", mixed_cols, hidden_all, preferred_element_type=jnp.float32
    )
    return (
        gate_weight_grad[None],
        up_weight_grad[None],
        down_grad[None],
        out_proj_grad,
        lru_input_grad,
    )


def solution(mesh):
    sp_count, tp_count = mesh.shape["sp"], mesh.shape["tp"]
    whole_blocks = 4 * SLICES == sp_count and tp_count == 4
    return jax.shard_map(
        direct if whole_blocks else local,
        mesh=mesh,
        in_specs=(
            P("sp", None),
            P("sp", None),
            P("sp", None),
            P("sp", None),
            P("sp", None, "tp"),
            P("sp", None, "tp"),
            P("sp", "tp", None),
            P("sp", "tp"),
            P("sp", "tp"),
            P("sp", "tp"),
            P("tp"),
            P("sp"),
            P("tp", None, None),
            P("tp", None, None),
        ),
        out_specs=(
            P("sp", None, "tp"),
            P("sp", None, "tp"),
            P("sp", "tp", None),
            P("sp", "tp"),
            P("sp", "tp"),
        ),
        check_vma=False,
    )
```

```python
import functools

import jax
import jax.numpy as jnp
from jax import lax
from jax.experimental import pallas as pl
from jax.experimental.pallas import tpu as pltpu
from jax.sharding import PartitionSpec as P

SLICES = 2


def prefix(part, axis, combine, identity):
    count = lax.axis_size(axis)
    place = lax.axis_index(axis)
    ahead = count - 1 - place
    gathered = jax.tree.map(lambda a: lax.all_gather(a, axis), part)
    state = jax.tree.map(lambda a, e: jnp.zeros_like(a) + jnp.asarray(e, a.dtype), part, identity)

    def one(turn, state):
        source = count - 1 - turn
        return combine(
            state, jax.tree.map(lambda a: lax.dynamic_index_in_dim(a, source, 0, False), gathered)
        )

    return lax.fori_loop(0, ahead, one, state)


def silu_slope(value):
    sig_value = jax.nn.sigmoid(value)
    return sig_value * (1.0 + value * (1.0 - sig_value))


def compose(upper_map, lower_map):
    return (lower_map[0] * upper_map[0], lower_map[1] + lower_map[0] * upper_map[1])


def chain_join(higher_map, lower_map):
    return (lower_map[0] * higher_map[0], lower_map[1] + lower_map[0] * higher_map[1])


def expert_backward(inputs, grads_in, gate_weight, up_weight, down_weight):
    gate_value = jnp.dot(inputs, gate_weight, preferred_element_type=jnp.float32)
    up_value = jnp.dot(inputs, up_weight, preferred_element_type=jnp.float32)
    active = jax.nn.silu(gate_value)
    hidden = (active * up_value).astype(jnp.bfloat16)
    down_grad = jnp.einsum(
        "rf,rd->fd", hidden, grads_in, preferred_element_type=jnp.float32
    ).astype(jnp.bfloat16)
    hidden_grad = jnp.einsum("rd,fd->rf", grads_in, down_weight, preferred_element_type=jnp.float32)
    gate_grad = (hidden_grad * up_value * silu_slope(gate_value)).astype(jnp.bfloat16)
    up_grad = (hidden_grad * active).astype(jnp.bfloat16)
    gate_weight_grad = jnp.einsum(
        "rd,rf->df", inputs, gate_grad, preferred_element_type=jnp.float32
    ).astype(jnp.bfloat16)
    up_weight_grad = jnp.einsum(
        "rd,rf->df", inputs, up_grad, preferred_element_type=jnp.float32
    ).astype(jnp.bfloat16)
    token_part = jnp.einsum("rf,df->rd", gate_grad, gate_weight, preferred_element_type=jnp.float32)
    token_part = token_part + jnp.einsum(
        "rf,df->rd", up_grad, up_weight, preferred_element_type=jnp.float32
    )
    return (gate_weight_grad, up_weight_grad, down_grad, token_part)


def collect(returned, targets, route_count):
    gathered = jnp.take(returned, targets[0], axis=0).astype(jnp.float32)
    for target in targets[1:]:
        gathered = gathered + jnp.take(returned, target, axis=0).astype(jnp.float32)
    return gathered.reshape(-1, route_count, gathered.shape[-1]).sum(axis=1)


def fill_slots(values, targets, slot_rows):
    buffer = jnp.zeros((slot_rows, values.shape[1]), jnp.bfloat16)
    for target in targets:
        buffer = buffer.at[target].set(values)
    return buffer


MESH_ID = pl.DeviceIdType.MESH


def greet(peers):
    barrier = pltpu.get_barrier_semaphore()
    for peer in peers:
        pl.semaphore_signal(barrier, inc=1, device_id=peer, device_id_type=MESH_ID)
    pl.semaphore_wait(barrier, len(peers))


def remote(src, dst, send, recv, peer):
    return pltpu.make_async_remote_copy(
        src_ref=src, dst_ref=dst, send_sem=send, recv_sem=recv, device_id=peer, device_id_type=MESH_ID
    )


def places(sp_count):
    me = lax.axis_index("sp")
    tp = lax.axis_index("tp")
    side, core = tp // 2, tp % 2
    peers = [(lax.rem(me + k, sp_count), tp) for k in range(sp_count)]
    sources = [lax.rem(me + sp_count - k, sp_count) for k in range(sp_count)]
    sibling = (me, side * 2 + (1 - core))
    across = (me, (1 - side) * 2 + core)
    return me, side, core, peers, sources, sibling, across


def gather_kernel(sp_count, x_ref, g_ref, info_ref, r_ref, h_ref, xo, go, io, ro, ho,
                  zs, zr, xs, xr, ys, yr, ss, sr, ts, tr, local_sem):
    me, side, core, peers, sources, sibling, across = places(sp_count)
    tp = lax.axis_index("tp")
    rows, feats = x_ref.shape
    half = feats // 2
    passed = 3 * half // 8
    direct = half - passed
    first = pl.multiple_of(core * half + side * passed, 128)
    onward = pl.multiple_of(core * half + side * direct, 128)
    back = pl.multiple_of(core * half + (1 - side) * direct, 128)
    depth = sp_count // 2
    z, x = me // 2, me % 2
    partner = (z * 2 + 1 - x, tp)
    along = [(lax.rem(z + k, depth) * 2 + x, tp) for k in range(depth)]
    line = [lax.rem(z + depth - k, depth) * 2 for k in range(depth)]

    def at(ref, who, col, width):
        return ref.at[pl.ds(pl.multiple_of(who * rows, rows), rows), pl.ds(col, width)]

    def block(ref, who, size):
        return ref.at[pl.ds(pl.multiple_of(who * size, size), size), :]

    greet(along[1:] + [partner, sibling, across])
    pairs = ((x_ref, xo), (g_ref, go))
    small = ((info_ref, io), (r_ref, ro), (h_ref, ho))
    waits = []
    recv = {}

    def send(key, src, dst, sems, index, peer):
        cp = remote(src, dst, sems[0].at[index], sems[1].at[index], peer)
        cp.start()
        recv[key] = cp

    for n, (src, dst) in enumerate(pairs + small):
        cp = pltpu.make_async_copy(src, block(dst, me, src.shape[0]), local_sem.at[n])
        cp.start()
        waits.append(cp)

    def open_pair(a):
        src, dst = pairs[a]
        for k in range(depth - 1, 0, -1):
            send(("z", a, k), src.at[:, pl.ds(first, direct)], at(dst, me, first, direct), (zs, zr), (a, k), along[k])
        send(("x", a, 0), src.at[:, pl.ds(first, direct)], at(dst, me, first, direct), (xs, xr), (a, 0), partner)

    def spread(a, who, n):
        dst = pairs[a][1]
        send(("y", a, n), at(dst, who, onward, passed), at(dst, who, onward, passed), (ys, yr), (a, n), across)
        send(("s", a, n), at(dst, who, first, direct), at(dst, who, first, direct), (ss, sr), (a, n), sibling)

    def open_small(b):
        src, dst = small[b]
        size = src.shape[0]
        for k in range(depth - 1, 0, -1):
            send(("z", 2 + b, k), src, block(dst, me, size), (zs, zr), (2 + b, k), along[k])
        send(("x", 2 + b, 0), src, block(dst, me, size), (xs, xr), (2 + b, 0), partner)

    open_pair(0)
    open_small(0)
    open_pair(1)
    open_small(1)
    open_small(2)
    for a in range(2):
        for k in range(1, depth):
            recv["z", a, k].wait_recv()
            who = line[k] + x
            dst = pairs[a][1]
            send(("x", a, k), at(dst, who, first, direct), at(dst, who, first, direct), (xs, xr), (a, k), partner)
            spread(a, who, k)
        for k in range(depth):
            recv["x", a, k].wait_recv()
            spread(a, line[k] + 1 - x, depth + k)
    for b in range(3):
        dst = small[b][1]
        size = small[b][0].shape[0]
        for k in range(1, depth):
            recv["z", 2 + b, k].wait_recv()
            who = line[k] + x
            send(("x", 2 + b, k), block(dst, who, size), block(dst, who, size), (xs, xr), (2 + b, k), partner)
    for a in range(2):
        dst = pairs[a][1]
        for n in range(1, 2 * depth):
            recv["y", a, n].wait_recv()
            who = line[n] + x if n < depth else line[n - depth] + 1 - x
            send(("t", a, n), at(dst, who, back, passed), at(dst, who, back, passed), (ts, tr), (a, n), sibling)
    for b in range(3):
        for k in range(depth):
            recv["x", 2 + b, k].wait_recv()
    for a in range(2):
        for n in range(1, 2 * depth):
            recv["s", a, n].wait_recv()
            recv["t", a, n].wait_recv()
    for cp in recv.values():
        cp.wait_send()
    for cp in waits:
        cp.wait()


def gather_all(sp_count, x, g, info, r, h):
    dma = pltpu.SemaphoreType.DMA
    outs = [jax.ShapeDtypeStruct((a.shape[0] * sp_count, a.shape[1]), a.dtype) for a in (x, g, info, r, h)]
    return pl.pallas_call(
        functools.partial(gather_kernel, sp_count),
        out_shape=outs,
        in_specs=[pl.BlockSpec(memory_space=pltpu.VMEM)] * 5,
        out_specs=[pl.BlockSpec(memory_space=pl.ANY)] * 5,
        scratch_shapes=[dma((5, sp_count))] * 4 + [dma((2, sp_count))] * 6 + [dma((5,))],
        compiler_params=pltpu.CompilerParams(collective_id=0, has_side_effects=True),
    )(x, g, info, r, h)


def return_kernel(sp_count, p_ref, g_ref, mixed, sib, out, ygot, last, got,
                  a_s, a_r, y_s, y_r, b_s, b_r, c_s, c_r):
    me, side, core, peers, sources, sibling, across = places(sp_count)
    rows, feats = g_ref.shape
    half, quarter = feats // 2, feats // 4
    mine = pl.multiple_of(core * half, half)
    theirs = pl.multiple_of((1 - core) * half, half)
    own = pl.ds(pl.multiple_of(side * quarter, quarter), quarter)
    other = pl.ds(pl.multiple_of((1 - side) * quarter, quarter), quarter)
    greet(peers[1:] + [sibling, across])
    order = list(range(sp_count // 2, 0, -1)) + list(range(sp_count // 2 + 1, sp_count)) + [0]
    first, second, third = {}, {}, {}
    for k in order:
        at = pl.ds(pl.multiple_of(peers[k][0] * rows, rows), rows)
        first[k] = remote(p_ref.at[at, pl.ds(theirs, half)], sib.at[k], a_s.at[k], a_r.at[k], sibling)
        first[k].start()
    for k in order:
        at = pl.ds(pl.multiple_of(peers[k][0] * rows, rows), rows)
        first[k].wait_recv()
        total = p_ref[at, pl.ds(mine, half)].astype(jnp.float32) + sib[k].astype(jnp.float32)
        out[k] = total.astype(jnp.bfloat16)
        second[k] = remote(out.at[k, :, other], ygot.at[k], y_s.at[k], y_r.at[k], across)
        second[k].start()
    for k in order:
        second[k].wait_recv()
        total = out[k, :, own].astype(jnp.float32) + ygot[k].astype(jnp.float32)
        last[k] = total.astype(jnp.bfloat16)
        if k:
            third[k] = remote(last.at[k], got.at[k], b_s.at[k], b_r.at[k], peers[k])
            third[k].start()
    total = last[0].astype(jnp.float32)
    for k in order[:-1]:
        third[k].wait_recv()
        total = total + got[k].astype(jnp.float32)
    here = pl.ds(pl.multiple_of(core * half + side * quarter, quarter), quarter)
    there = pl.ds(pl.multiple_of(core * half + (1 - side) * quarter, quarter), quarter)
    mixed[:, here] = (g_ref[:, here].astype(jnp.float32) + total).astype(jnp.bfloat16)
    ends = []
    for n, (cols, who) in enumerate(((here, across), (here, sibling), (there, sibling))):
        if n == 2:
            ends[0].wait_recv()
        cp = remote(mixed.at[:, cols], mixed.at[:, cols], c_s.at[n], c_r.at[n], who)
        cp.start()
        ends.append(cp)
    ends[1].wait_recv()
    ends[2].wait_recv()
    for cp in ends + list(first.values()) + list(second.values()) + list(third.values()):
        cp.wait_send()


def return_all(sp_count, partial, g):
    dma = pltpu.SemaphoreType.DMA
    rows, feats = g.shape
    big = pltpu.VMEM((sp_count, rows, feats // 2), jnp.bfloat16)
    small = pltpu.VMEM((sp_count, rows, feats // 4), jnp.bfloat16)
    return pl.pallas_call(
        functools.partial(return_kernel, sp_count),
        out_shape=jax.ShapeDtypeStruct((rows, feats), jnp.bfloat16),
        in_specs=[pl.BlockSpec(memory_space=pltpu.VMEM)] * 2,
        out_specs=pl.BlockSpec(memory_space=pltpu.VMEM),
        scratch_shapes=[big, big, small, small, small] + [dma((sp_count,))] * 6 + [dma((3,))] * 2,
        compiler_params=pltpu.CompilerParams(collective_id=1, has_side_effects=True),
    )(partial, g)


def carry_kernel(sp_count, mixed, decay_ref, up_ref, dstate, cols_out, block, got, s, r, d_s, d_r, local_sem):
    me, side, core, peers, sources, sibling, across = places(sp_count)
    rows, feats = mixed.shape
    width = feats // sp_count
    greet(peers[1:])
    own = pl.ds(pl.multiple_of(me * rows, rows), rows)
    moved = []
    for k in range(1, sp_count):
        cols = pl.ds(pl.multiple_of(peers[k][0] * width, width), width)
        cp = remote(mixed.at[:, cols], cols_out.at[own, :], d_s.at[k], d_r.at[k], peers[k])
        cp.start()
        moved.append(cp)
    here = pltpu.make_async_copy(
        mixed.at[:, pl.ds(pl.multiple_of(me * width, width), width)], cols_out.at[own, :], local_sem
    )
    here.start()
    row = lax.broadcasted_iota(jnp.int32, up_ref.shape, 0)
    decay = decay_ref[...]
    prod = jnp.where(row < rows - 1, pltpu.roll(decay, rows - 1, 0), 1.0)
    part = up_ref[...]
    step = 1
    while step < rows:
        keep = row < rows - step
        later = jnp.where(keep, pltpu.roll(part, rows - step, 0), 0.0)
        after = jnp.where(keep, pltpu.roll(prod, rows - step, 0), 1.0)
        part = part + prod * later
        prod = prod * after
        step *= 2
    block[...] = jnp.zeros_like(block)
    got[me] = jnp.zeros(block.shape, jnp.float32)
    block[0:1] = decay[0:1] * prod[0:1]
    block[1:2] = decay[0:1] * part[0:1]
    copies = []
    for k in range(1, sp_count):
        cp = remote(block, got.at[me], s.at[k], r.at[k], peers[k])
        cp.start()
        copies.append(cp)
    for cp in copies:
        cp.wait()
    incoming = jnp.zeros((1, up_ref.shape[1]), jnp.float32)
    for source in range(sp_count - 1, 0, -1):
        value = got[source]
        incoming = jnp.where(source > me, value[1:2] + value[0:1] * incoming, incoming)
    dstate[...] = part + prod * incoming
    here.wait()
    for cp in moved:
        cp.wait()


def carry_all(sp_count, mixed, decay, upstream):
    dma = pltpu.SemaphoreType.DMA
    rows, feats = mixed.shape
    block = (8, upstream.shape[1])
    return pl.pallas_call(
        functools.partial(carry_kernel, sp_count),
        out_shape=[
            jax.ShapeDtypeStruct(upstream.shape, jnp.float32),
            jax.ShapeDtypeStruct((rows * sp_count, feats // sp_count), jnp.bfloat16),
        ],
        in_specs=[pl.BlockSpec(memory_space=pltpu.VMEM)] * 3,
        out_specs=[pl.BlockSpec(memory_space=pltpu.VMEM)] * 2,
        scratch_shapes=[pltpu.VMEM(block, jnp.float32), pltpu.VMEM((sp_count,) + block, jnp.float32)]
        + [dma((sp_count,))] * 4
        + [dma],
        compiler_params=pltpu.CompilerParams(collective_id=2, has_side_effects=True),
    )(mixed, decay, upstream)


def local(
    result_cotangent_values,
    specialist_entry_vectors,
    chosen_specialists,
    specialist_mixing_shares,
    specialist_switch_maps,
    specialist_widen_maps,
    specialist_shrink_maps,
    memory_readout_map,
    memory_source_vectors,
    memory_hidden_values,
    feature_fading_speed,
    extra_log_fading,
    memory_switch_tiles,
    entry_switch_tiles,
):
    tok_rows, feature_count = result_cotangent_values.shape
    route_count = chosen_specialists.shape[1]
    sp_count = lax.axis_size("sp")
    expert_count = sp_count // SLICES
    capacity = min(tok_rows, 4 * tok_rows // expert_count)
    slot_rows = sp_count * capacity
    flat_expert = chosen_specialists.reshape(-1)
    onehot = (flat_expert[:, None] == jnp.arange(expert_count, dtype=jnp.int32)[None, :]).astype(
        jnp.int32
    )
    slot_rank = jnp.sum((jnp.cumsum(onehot, axis=0) - 1) * onehot, axis=1)
    scaled = (
        (
            specialist_mixing_shares[:, :, None]
            * result_cotangent_values[:, None, :].astype(jnp.float32)
        )
        .astype(jnp.bfloat16)
        .reshape(-1, feature_count)
    )
    copies = jnp.broadcast_to(
        specialist_entry_vectors[:, None, :], (tok_rows, route_count, feature_count)
    ).reshape(-1, feature_count)
    targets = [
        (flat_expert * SLICES + slice_index) * capacity + slot_rank for slice_index in range(SLICES)
    ]
    share = feature_count // lax.axis_size("tp")
    first_col = lax.axis_index("tp") * share
    part_grad = lax.dynamic_slice_in_dim(scaled, first_col, share, 1)
    part_rows = lax.dynamic_slice_in_dim(copies, first_col, share, 1)
    send_grad = fill_slots(part_grad, targets, slot_rows)
    send_rows = fill_slots(part_rows, targets, slot_rows)
    got_grad, got_rows = (
        lax.all_to_all(
            send_grad.reshape(sp_count, capacity, share),
            "sp",
            split_axis=0,
            concat_axis=0,
            tiled=True,
        ),
        lax.all_to_all(
            send_rows.reshape(sp_count, capacity, share),
            "sp",
            split_axis=0,
            concat_axis=0,
            tiled=True,
        ),
    )
    recv_grad, recv_rows = (
        lax.all_gather(got_grad, "tp", axis=2, tiled=True),
        lax.all_gather(got_rows, "tp", axis=2, tiled=True),
    )
    inputs = recv_rows.reshape(slot_rows, feature_count)
    grads_in = recv_grad.reshape(slot_rows, feature_count)
    gate_weight_grad, up_weight_grad, down_grad, token_part = expert_backward(
        inputs,
        grads_in,
        specialist_switch_maps[0],
        specialist_widen_maps[0],
        specialist_shrink_maps[0],
    )
    returned = lax.all_to_all(
        token_part.astype(jnp.bfloat16).reshape(sp_count, capacity, feature_count),
        "sp",
        split_axis=0,
        concat_axis=0,
        tiled=True,
    )
    own_sum = collect(returned.reshape(slot_rows, feature_count), targets, route_count)
    moe_grad = lax.psum(own_sum.astype(jnp.bfloat16), "tp").astype(jnp.float32)
    mixed_grad = (result_cotangent_values.astype(jnp.float32) + moe_grad).astype(jnp.bfloat16)
    col_count = memory_readout_map.shape[1]
    columns = mixed_grad
    upstream = jnp.dot(
        columns,
        lax.all_gather(memory_readout_map, "sp", axis=0, tiled=True),
        preferred_element_type=jnp.float32,
    )
    blocks_here = memory_switch_tiles.shape[0]
    block_width = memory_switch_tiles.shape[1]
    blocks_in = memory_source_vectors.reshape(tok_rows, blocks_here, block_width)
    memory_switch_fraction = jax.nn.sigmoid(
        jnp.einsum(
            "tnc,ncd->tnd", blocks_in, memory_switch_tiles, preferred_element_type=jnp.float32
        ).reshape(tok_rows, col_count)
    )
    inp_open = jax.nn.sigmoid(
        jnp.einsum(
            "tnc,ncd->tnd", blocks_in, entry_switch_tiles, preferred_element_type=jnp.float32
        ).reshape(tok_rows, col_count)
    )
    xin = memory_source_vectors.astype(jnp.float32)
    log_fading_factor = (
        -8.0 * memory_switch_fraction * feature_fading_speed[None, :] + extra_log_fading[:, None]
    )
    decay_mult = jnp.exp(log_fading_factor)
    spare_room = -jnp.expm1(2.0 * log_fading_factor)
    in_scale = jnp.sqrt(jnp.maximum(spare_room, 0.01))
    drive = in_scale * inp_open * xin
    coeff = jnp.concatenate([decay_mult[1:], jnp.ones((1, col_count), jnp.float32)], axis=0)
    prod_after, local_part = lax.associative_scan(compose, (coeff, upstream), reverse=True, axis=0)
    alpha_part = decay_mult[0] * local_part[0]
    beta_part = decay_mult[0] * prod_after[0]
    carried = prefix(
        (beta_part, alpha_part),
        "sp",
        chain_join,
        (jnp.ones_like(beta_part), jnp.zeros_like(alpha_part)),
    )
    incoming = carried[1]
    dstate = local_part + prod_after * incoming[None, :]
    scale_slope = jnp.where(spare_room > 0.01, -decay_mult * decay_mult / in_scale, 0.0)
    log_grad = dstate * (
        memory_hidden_values.astype(jnp.float32) - drive + scale_slope * inp_open * xin
    )
    grad_rec = (
        log_grad
        * (-8.0 * feature_fading_speed[None, :])
        * memory_switch_fraction
        * (1.0 - memory_switch_fraction)
    ).astype(jnp.bfloat16)
    grad_in = (dstate * in_scale * xin * inp_open * (1.0 - inp_open)).astype(jnp.bfloat16)
    back_rec = jnp.einsum(
        "tnd,ncd->tnc",
        grad_rec.reshape(tok_rows, blocks_here, block_width),
        memory_switch_tiles,
        preferred_element_type=jnp.float32,
    )
    back_in = jnp.einsum(
        "tnd,ncd->tnc",
        grad_in.reshape(tok_rows, blocks_here, block_width),
        entry_switch_tiles,
        preferred_element_type=jnp.float32,
    )
    lru_input_grad = (
        dstate * in_scale * inp_open
        + back_rec.reshape(tok_rows, col_count)
        + back_in.reshape(tok_rows, col_count)
    )
    columns = mixed_grad
    out_proj_grad = lax.psum_scatter(
        jnp.einsum("tr,tc->rc", columns, memory_hidden_values, preferred_element_type=jnp.float32),
        "sp",
        scatter_dimension=0,
        tiled=True,
    )
    return (
        gate_weight_grad[None],
        up_weight_grad[None],
        down_grad[None],
        out_proj_grad,
        lru_input_grad,
    )


def direct(
    result_cotangent_values,
    specialist_entry_vectors,
    chosen_specialists,
    specialist_mixing_shares,
    specialist_switch_maps,
    specialist_widen_maps,
    specialist_shrink_maps,
    memory_readout_map,
    memory_source_vectors,
    memory_hidden_values,
    feature_fading_speed,
    extra_log_fading,
    memory_switch_tiles,
    entry_switch_tiles,
):
    tok_rows, feature_count = result_cotangent_values.shape
    sp_count = lax.axis_size("sp")
    info = jnp.concatenate(
        [
            chosen_specialists.astype(jnp.float32).T,
            specialist_mixing_shares.T,
            jnp.zeros((4, tok_rows), jnp.float32),
        ],
        axis=0,
    )
    inputs, all_grad, info, readout, hidden_all = gather_all(
        sp_count,
        specialist_entry_vectors,
        result_cotangent_values,
        info,
        memory_readout_map,
        memory_hidden_values,
    )
    expert = (lax.axis_index("sp") // SLICES).astype(jnp.float32)
    info = info.reshape(sp_count, 8, tok_rows)
    share = jnp.where(info[:, 0] == expert, info[:, 2], 0.0) + jnp.where(
        info[:, 1] == expert, info[:, 3], 0.0
    )
    grads_in = (share.reshape(-1, 1) * all_grad.astype(jnp.float32)).astype(jnp.bfloat16)
    gate_weight_grad, up_weight_grad, down_grad, token_part = expert_backward(
        inputs,
        grads_in,
        specialist_switch_maps[0],
        specialist_widen_maps[0],
        specialist_shrink_maps[0],
    )
    mixed_grad = return_all(
        sp_count, token_part.astype(jnp.bfloat16), result_cotangent_values
    )
    col_count = memory_readout_map.shape[1]
    upstream = jnp.dot(mixed_grad, readout, preferred_element_type=jnp.float32)
    blocks_here = memory_switch_tiles.shape[0]
    block_width = memory_switch_tiles.shape[1]
    blocks_in = memory_source_vectors.reshape(tok_rows, blocks_here, block_width)
    memory_switch_fraction = jax.nn.sigmoid(
        jnp.einsum(
            "tnc,ncd->tnd", blocks_in, memory_switch_tiles, preferred_element_type=jnp.float32
        ).reshape(tok_rows, col_count)
    )
    inp_open = jax.nn.sigmoid(
        jnp.einsum(
            "tnc,ncd->tnd", blocks_in, entry_switch_tiles, preferred_element_type=jnp.float32
        ).reshape(tok_rows, col_count)
    )
    xin = memory_source_vectors.astype(jnp.float32)
    log_fading_factor = (
        -8.0 * memory_switch_fraction * feature_fading_speed[None, :] + extra_log_fading[:, None]
    )
    decay_mult = jnp.exp(log_fading_factor)
    spare_room = -jnp.expm1(2.0 * log_fading_factor)
    in_scale = jnp.sqrt(jnp.maximum(spare_room, 0.01))
    drive = in_scale * inp_open * xin
    dstate, mixed_cols = carry_all(sp_count, mixed_grad, decay_mult, upstream)
    scale_slope = jnp.where(spare_room > 0.01, -decay_mult * decay_mult / in_scale, 0.0)
    log_grad = dstate * (
        memory_hidden_values.astype(jnp.float32) - drive + scale_slope * inp_open * xin
    )
    grad_rec = (
        log_grad
        * (-8.0 * feature_fading_speed[None, :])
        * memory_switch_fraction
        * (1.0 - memory_switch_fraction)
    ).astype(jnp.bfloat16)
    grad_in = (dstate * in_scale * xin * inp_open * (1.0 - inp_open)).astype(jnp.bfloat16)
    back_rec = jnp.einsum(
        "tnd,ncd->tnc",
        grad_rec.reshape(tok_rows, blocks_here, block_width),
        memory_switch_tiles,
        preferred_element_type=jnp.float32,
    )
    back_in = jnp.einsum(
        "tnd,ncd->tnc",
        grad_in.reshape(tok_rows, blocks_here, block_width),
        entry_switch_tiles,
        preferred_element_type=jnp.float32,
    )
    lru_input_grad = (
        dstate * in_scale * inp_open
        + back_rec.reshape(tok_rows, col_count)
        + back_in.reshape(tok_rows, col_count)
    )
    out_proj_grad = jnp.einsum(
        "tr,tc->rc", mixed_cols, hidden_all, preferred_element_type=jnp.float32
    )
    return (
        gate_weight_grad[None],
        up_weight_grad[None],
        down_grad[None],
        out_proj_grad,
        lru_input_grad,
    )


def solution(mesh):
    sp_count, tp_count = mesh.shape["sp"], mesh.shape["tp"]
    whole_blocks = 4 * SLICES == sp_count and tp_count == 4
    return jax.shard_map(
        direct if whole_blocks else local,
        mesh=mesh,
        in_specs=(
            P("sp", None),
            P("sp", None),
            P("sp", None),
            P("sp", None),
            P("sp", None, "tp"),
            P("sp", None, "tp"),
            P("sp", "tp", None),
            P("sp", "tp"),
            P("sp", "tp"),
            P("sp", "tp"),
            P("tp"),
            P("sp"),
            P("tp", None, None),
            P("tp", None, None),
        ),
        out_specs=(
            P("sp", None, "tp"),
            P("sp", None, "tp"),
            P("sp", "tp", None),
            P("sp", "tp"),
            P("sp", "tp"),
        ),
        check_vma=False,
    )
```
